512 devices in a mesh: sp: 16 (over z), fs: 4 (over y), tp: 8 (over x, core).
Axes of the slice: x: 4, y: 4, z: 16, core: 2. Of those that a mesh axis runs over, the one named last changes fastest.
Arguments:
- tokens: bfloat16 [4, 8192, 2048], P('fs', 'sp'), may hold values from -6 to 6
- input_gain: float32 [2048], replicated, may hold values from 0.1 to 1.9
- weight_gate: bfloat16 [2048, 2048], P('sp', 'tp'), may hold values from -0.125 to 0.125
- weight_input: bfloat16 [2048, 2048], P('sp', 'tp'), may hold values from -0.125 to 0.125
- weight_write: bfloat16 [2048, 1024], P('sp', 'tp'), may hold values from -0.125 to 0.125
- weight_read: bfloat16 [2048, 1024], P('sp', 'tp'), may hold values from -0.125 to 0.125
- weight_step: bfloat16 [2048, 32], P('sp', 'tp'), may hold values from -0.125 to 0.125
- weight_value: bfloat16 [2048, 2048], P('sp', 'tp'), may hold values from -0.125 to 0.125
- weight_sigmoid: bfloat16 [2048, 2048], P('sp', 'tp'), may hold values from -0.125 to 0.125
- filter_input: bfloat16 [4, 2048], P(None, 'tp'), may hold values from -3 to 3
- filter_write: bfloat16 [4, 1024], P(None, 'tp'), may hold values from -3 to 3
- filter_read: bfloat16 [4, 1024], P(None, 'tp'), may hold values from -3 to 3
- step_bias: float32 [32], P('tp'), may hold values from -4.5 to -3.5
- rate_log: float32 [32], P('tp'), as said below
- skip_gain: float32 [32], P('tp'), may hold values from 0.1 to 1.9
- output_gain: float32 [2048], P('tp'), may hold values from 0.1 to 1.9
- opening_state: float32 [4, 32, 64, 128], P('fs', 'tp'), may hold values from -12 to 12
- decay_shift: float32 [4, 32, 8192], P('fs', 'tp', 'sp'), may hold values from -3 to 0, as said below
- depth_filter: bfloat16 [31, 2048], P(None, 'tp'), may hold values from -40 to 40
- channel_gain: float32 [2048], P('tp'), may hold values from 0.1 to 1.9
- unproject_state: bfloat16 [2048, 2048], P('tp', 'sp'), may hold values from -0.09375 to 0.09375
- unproject_filter: bfloat16 [2048, 2048], P('tp', 'sp'), may hold values from -0.09375 to 0.09375
Outputs:
- mixed: bfloat16 [4, 8192, 2048], P('fs', ('sp', 'tp'))
The draws below stay inside these ranges and needn't reach their ends.
Inputs may be any that keep to these rules, and one draw needn't show every extreme that they name: `rate_log`: logarithms of the heads' decay rates. `decay_shift`: Non-positive.
All inputs are finite; a program needn't handle non-finite values.
Results may differ from the reference program's by a relative error of at most 0.018.
Values may be sent and summed in bfloat16 or wider, within the bound.
A program may use at most 64 MiB of HBM per device.

```python
import math
from functools import partial
import jax
import jax.numpy as jnp
from jax import lax

D = 2048
HEADS = 32
HEAD_DIM = 64
GROUPS = 8
STATE = 128
CM = 2048
SSD_CONV = 4
CONV_SPAN = 31
BLOCK = 128
TOK_DEV = 512
SSD_WIDTH = 2048
SEQS = 4
LENGTH = 8192
N_TP = 8


def draw_rate_log(key, part):
    pick_key, slow_key, fast_key = jax.random.split(jax.random.fold_in(key, 11), 3)
    slow_share = 0.5
    slow_heads = jax.random.uniform(pick_key, (HEADS,), jnp.float32) < slow_share
    slow_rate = jnp.exp(jax.random.uniform(slow_key, (HEADS,), jnp.float32, math.log(10.0), math.log(33.0))) / LENGTH
    fast_rate = jnp.exp(jax.random.uniform(fast_key, (HEADS,), jnp.float32, math.log(0.7), math.log(1.5)))
    return jnp.log(jnp.where(slow_heads, slow_rate, fast_rate)).astype(jnp.float32)


def draw_decay_shift(key, part):
    factor_key, spot_key, depth_key, noise_key = jax.random.split(jax.random.fold_in(key, 23), 4)
    lowest = math.log(0.5)
    factors = jnp.exp(jax.random.uniform(factor_key, (SEQS, LENGTH // TOK_DEV), jnp.float32, lowest, math.log(2.0)))
    background_intensity = -(0.3 / LENGTH) * jnp.repeat(factors, TOK_DEV, axis=1)
    stochastic_perturbation = jax.random.uniform(noise_key, (SEQS, HEADS, LENGTH), jnp.float32, 0.5, 1.5)
    selected_locations = jax.random.randint(spot_key, (SEQS, 4), 0, LENGTH)
    kernel_channel_counts = jnp.log(jax.random.uniform(depth_key, (SEQS, 4), jnp.float32, 0.5, 0.8))
    sequence_indices = jnp.arange(LENGTH, dtype=jnp.int32)
    spike_occurrences = jnp.sum(jnp.where(sequence_indices[None, None, :] == selected_locations[:, :, None], kernel_channel_counts[:, :, None], 0.0), axis=1)
    return (background_intensity[:, None, :] * stochastic_perturbation + spike_occurrences[:, None, :]).astype(jnp.float32)


def draw_depth_filter(key, part):
    value_key, scale_key = jax.random.split(jax.random.fold_in(key, 37), 2)
    top_scale = math.log(10.0)
    ramp = jnp.arange(CM, dtype=jnp.float32) / (CM - 1)
    scales = jnp.exp(ramp * top_scale) * jnp.exp(jax.random.uniform(scale_key, (CM,), jnp.float32, 0.0, math.log(1.5)))
    values = jax.random.truncated_normal(value_key, -4.0, 4.0, (CONV_SPAN, CM), jnp.float32)
    return (values * scales[None, :] / math.sqrt(CONV_SPAN)).astype(jnp.bfloat16)


def block_levels(key, extent, cuts, low, largest):
    loudness, own = 1.0, jax.random.fold_in(key, 6)
    for axis_at, parts in cuts:
        steps = jnp.exp(jax.random.uniform(jax.random.fold_in(own, axis_at), (parts,), jnp.float32, low / len(cuts), largest / len(cuts)))
        loudness = loudness * jnp.repeat(steps, extent[axis_at] // parts).reshape([-1 if axis == axis_at else 1 for axis in range(len(extent))])
    return loudness


def normal_values(key, dims, scale, most, cuts=(), held_as=jnp.bfloat16):
    gain = block_levels(key, dims, cuts, -0.22, 0.18) if cuts else 1.0
    values = jax.random.normal(key, dims, jnp.float32) * scale * gain
    return jnp.minimum(jnp.maximum(values, -most), most).astype(held_as)


def setup_inputs(seed: int = 0) -> dict:
    streams_of = jax.random.split(jax.random.key(seed), 23)
    return {
        "tokens": normal_values(streams_of[0], (SEQS, LENGTH, D), 1.0, 6.0, ((0, 4), (1, 16))),
        "input_gain": jnp.clip(1.0 + 0.18 * jax.random.normal(streams_of[1], (D,), jnp.float32), 0.1, 1.9),
        "weight_gate": normal_values(streams_of[2], (D, SSD_WIDTH), D ** -0.5, 0.125, ((0, 16), (1, 8))),
        "weight_input": normal_values(streams_of[3], (D, SSD_WIDTH), D ** -0.5, 0.125, ((0, 16), (1, 8))),
        "weight_write": normal_values(streams_of[4], (D, GROUPS * STATE), D ** -0.5, 0.125, ((0, 16), (1, 8))),
        "weight_read": normal_values(streams_of[5], (D, GROUPS * STATE), D ** -0.5, 0.125, ((0, 16), (1, 8))),
        "weight_step": normal_values(streams_of[6], (D, HEADS), D ** -0.5, 0.125, ((0, 16), (1, 8))),
        "weight_value": normal_values(streams_of[7], (D, CM), D ** -0.5, 0.125, ((0, 16), (1, 8))),
        "weight_sigmoid": normal_values(streams_of[8], (D, CM), D ** -0.5, 0.125, ((0, 16), (1, 8))),
        "filter_input": normal_values(streams_of[9], (SSD_CONV, SSD_WIDTH), SSD_CONV ** -0.5, 3.0, ((1, 8),)),
        "filter_write": normal_values(streams_of[10], (SSD_CONV, GROUPS * STATE), SSD_CONV ** -0.5, 3.0, ((1, 8),)),
        "filter_read": normal_values(streams_of[11], (SSD_CONV, GROUPS * STATE), SSD_CONV ** -0.5, 3.0, ((1, 8),)),
        "step_bias": jnp.clip(-4.5 + 1.0 * jax.random.uniform(streams_of[12], (HEADS,), jnp.float32) ** block_levels(streams_of[12], (HEADS,), ((0, 8),), -0.2, 0.2), -4.5, -3.5),
        "rate_log": draw_rate_log(jax.random.fold_in(streams_of[22], 71), 0),
        "skip_gain": jnp.clip(1.0 + 0.18 * jax.random.normal(streams_of[14], (HEADS,), jnp.float32), 0.1, 1.9),
        "output_gain": jnp.clip(1.0 + 0.18 * jax.random.normal(streams_of[15], (SSD_WIDTH,), jnp.float32), 0.1, 1.9),
        "opening_state": normal_values(streams_of[16], (SEQS, HEADS, HEAD_DIM, STATE), 2.0, 12.0, ((0, 4), (1, 8)), jnp.float32),
        "decay_shift": draw_decay_shift(jax.random.fold_in(streams_of[22], 71), 0),
        "depth_filter": draw_depth_filter(jax.random.fold_in(streams_of[22], 71), 0),
        "channel_gain": jnp.clip(1.0 + 0.18 * jax.random.normal(streams_of[19], (CM,), jnp.float32), 0.1, 1.9),
        "unproject_state": normal_values(streams_of[20], (SSD_WIDTH, D), (SSD_WIDTH + CM) ** -0.5, 0.09375, ((0, 8), (1, 16))),
        "unproject_filter": normal_values(streams_of[21], (CM, D), (SSD_WIDTH + CM) ** -0.5, 0.09375, ((0, 8), (1, 16))),
    }


exact_mode = lax.Precision.HIGHEST

def causal_filter(border, values, kernel):
    extended = jnp.concatenate([border, values], axis=0).astype(jnp.float32)
    weights = kernel.astype(jnp.float32)
    row_count = values.shape[0]
    result = jnp.zeros(values.shape, jnp.float32)
    for offset in range(kernel.shape[0]):
        result = result + weights[offset] * extended[offset:offset + row_count]
    return result

def block_step(direct_gain, memory, pieces):
    input_block, write_block, read_block, step_block, log_block = pieces
    head_count = input_block.shape[1]
    per_group = head_count // write_block.shape[1]
    running = jnp.cumsum(log_block, axis=0)
    write_heads = jnp.repeat(write_block, per_group, axis=1)
    read_heads = jnp.repeat(read_block, per_group, axis=1)
    scores = jnp.einsum('lhn,shn->hls', read_heads, write_heads, precision=exact_mode)
    spread = running.T[:, :, None] - running.T[:, None, :]
    row_index = lax.broadcasted_iota(jnp.int32, spread.shape, 1)
    col_index = lax.broadcasted_iota(jnp.int32, spread.shape, 2)
    decays = jnp.exp(jnp.where(row_index >= col_index, spread, -jnp.inf))
    scaled_inputs = input_block * step_block[:, :, None]
    inside = jnp.einsum('hls,shp->lhp', scores * decays, scaled_inputs, precision=exact_mode)
    carried = jnp.exp(running)[:, :, None] * jnp.einsum('lhn,hpn->lhp', read_heads, memory, precision=exact_mode)
    output = inside + carried + direct_gain[None, :, None] * input_block
    to_end = jnp.exp(running[-1][None, :] - running)
    fresh_terms = jnp.einsum('lhp,lhn->hpn', scaled_inputs * to_end[:, :, None], write_heads, precision=exact_mode)
    new_memory = jnp.exp(running[-1])[:, None, None] * memory + fresh_terms
    return (new_memory, output)

def reference(tokens, input_gain, weight_gate, weight_input, weight_write, weight_read, weight_step, weight_value, weight_sigmoid, filter_input, filter_write, filter_read, step_bias, rate_log, skip_gain, output_gain, opening_state, decay_shift, depth_filter, channel_gain, unproject_state, unproject_filter):

    def project(normed, weight):
        return jnp.dot(normed, weight, preferred_element_type=jnp.float32).astype(jnp.bfloat16)

    def one_sequence(packed):
        sequence, start_memory, shift_rows = packed
        source = sequence.astype(jnp.float32)
        normed = (source * lax.rsqrt(lax.optimization_barrier(jnp.mean(source * source, axis=-1, keepdims=True)) + 1e-06) * input_gain).astype(jnp.bfloat16)
        gate_values = project(normed, weight_gate)
        input_values = project(normed, weight_input)
        write_values = project(normed, weight_write)
        read_values = project(normed, weight_read)
        step_values = project(normed, weight_step)
        value_rows = project(normed, weight_value)
        sigmoid_rows = project(normed, weight_sigmoid)
        glu_rows = (value_rows.astype(jnp.float32) * jax.nn.sigmoid(sigmoid_rows.astype(jnp.float32))).astype(jnp.bfloat16)
        short_rim = SSD_CONV - 1
        mixed_input = jax.nn.silu(causal_filter(jnp.zeros((short_rim, SSD_WIDTH), jnp.bfloat16), input_values, filter_input)).astype(jnp.bfloat16)
        mixed_write = jax.nn.silu(causal_filter(jnp.zeros((short_rim, GROUPS * STATE), jnp.bfloat16), write_values, filter_write)).astype(jnp.bfloat16)
        mixed_read = jax.nn.silu(causal_filter(jnp.zeros((short_rim, GROUPS * STATE), jnp.bfloat16), read_values, filter_read)).astype(jnp.bfloat16)
        step_sizes = jax.nn.softplus(step_values.astype(jnp.float32) + step_bias)
        log_rates = -step_sizes * jnp.exp(rate_log) + shift_rows.T
        block_count = LENGTH // BLOCK
        inputs_float = mixed_input.astype(jnp.float32).reshape(block_count, BLOCK, HEADS, HEAD_DIM)
        write_float = mixed_write.astype(jnp.float32).reshape(block_count, BLOCK, GROUPS, STATE)
        read_float = mixed_read.astype(jnp.float32).reshape(block_count, BLOCK, GROUPS, STATE)
        blocked = (inputs_float, write_float, read_float, step_sizes.reshape(block_count, BLOCK, HEADS), log_rates.reshape(block_count, BLOCK, HEADS))
        final_memory, outputs = lax.scan(partial(block_step, skip_gain), start_memory, blocked)
        gated = outputs.reshape(LENGTH, SSD_WIDTH) * jax.nn.silu(gate_values.astype(jnp.float32))
        grouped = gated.reshape(LENGTH, GROUPS, SSD_WIDTH // GROUPS)
        grouped = grouped * lax.rsqrt(lax.optimization_barrier(jnp.mean(grouped * grouped, axis=-1, keepdims=True)) + 1e-06)
        state_out = (grouped.reshape(LENGTH, SSD_WIDTH) * output_gain).astype(jnp.bfloat16)
        filtered = causal_filter(jnp.zeros((CONV_SPAN - 1, CM), jnp.bfloat16), glu_rows, depth_filter)
        mean_value = lax.optimization_barrier(jnp.mean(filtered, axis=-1, keepdims=True))
        mean_square = lax.optimization_barrier(jnp.mean(filtered * filtered, axis=-1, keepdims=True))
        variance = mean_square - mean_value * mean_value
        filter_out = jax.nn.silu((filtered - mean_value) * lax.rsqrt(variance + 1e-05) * channel_gain).astype(jnp.bfloat16)
        state_width = SSD_WIDTH // N_TP
        filter_width = CM // N_TP

        def add_term(total, block_index):
            state_cols = lax.dynamic_slice_in_dim(state_out, block_index * state_width, state_width, 1)
            state_weights = lax.dynamic_slice_in_dim(unproject_state, block_index * state_width, state_width, 0)
            filter_cols = lax.dynamic_slice_in_dim(filter_out, block_index * filter_width, filter_width, 1)
            filter_weights = lax.dynamic_slice_in_dim(unproject_filter, block_index * filter_width, filter_width, 0)
            term = jnp.dot(state_cols, state_weights, preferred_element_type=jnp.float32)
            term = term + jnp.dot(filter_cols, filter_weights, preferred_element_type=jnp.float32)
            rounded = lax.optimization_barrier(term.astype(jnp.bfloat16))
            return (total + rounded.astype(jnp.float32), None)
        total, unused = lax.scan(add_term, jnp.zeros((LENGTH, D), jnp.float32), jnp.arange(N_TP, dtype=jnp.int32))
        return total.astype(jnp.bfloat16)
    return lax.map(one_sequence, (tokens, opening_state, decay_shift))
```

```python
from functools import partial

import jax
import jax.numpy as jnp
from jax import lax
from jax.experimental import pallas as pl
from jax.experimental.pallas import tpu as pltpu
from jax.sharding import PartitionSpec as P

HEAD_DIM = 64
STATE = 128
CM = 2048
BLOCK = 128


MESH = pl.DeviceIdType.MESH


def gather_project_kernel(
    n, offsets,
    tok, gain, wi, ww, ws, wg, wr, wv, wsg, us, uf,
    o_gate, o_inp, o_wr, o_rd, o_step, o_glu, o_us, o_uf,
    normed, ap, aq, as_, bp, bq, cp, acc_a, acc_s, acc_b, acc_c,
    local_sem, zs, zr, ys, yr,
):
    z = lax.axis_index("sp")
    y = lax.axis_index("fs")
    n_right, n_left = n // 2, (n - 1) // 2
    z_next, z_prev = lax.rem(z + 1, n), lax.rem(z + n - 1, n)
    y_next, y_prev = lax.rem(y + 1, 4), lax.rem(y + 3, 4)

    pairs = [
        (wi, ap.at[z]), (ww, aq.at[z]), (ws, as_.at[z]), (wg, bp.at[z]), (wr, bq.at[z]),
        (wv, cp.at[z, :, pl.ds(0, 256)]), (wsg, cp.at[z, :, pl.ds(256, 256)]),
        (us, o_us.at[z]), (uf, o_uf.at[z]),
    ]
    own = [pltpu.make_async_copy(s, d, local_sem.at[k]) for k, (s, d) in enumerate(pairs)]
    for c in own:
        c.start()
    barrier = pltpu.get_barrier_semaphore()
    for where in ({"sp": z_next}, {"sp": z_prev}, {"fs": y_next}, {"fs": y_prev}):
        pl.semaphore_signal(barrier, inc=1, device_id=where, device_id_type=MESH)
    for c in own:
        c.wait()
    pl.semaphore_wait(barrier, 4)

    groups = [((ap,), (aq, as_)), ((bp,), (bq,)), ((cp,), ()), ((o_us,), (o_uf,))]
    zbase, ybase, zi, yi = [], [], 0, 0
    for two, one in groups:
        zbase.append(zi)
        ybase.append(yi)
        zi += len(two) + len(one)
        yi += len(two)

    def shard(s, way):
        return lax.rem(z + n - s, n) if way == 0 else lax.rem(z + s, n)

    def part(buf, j, q):
        rows = buf.shape[1] // 4
        return buf.at[j, pl.ds(pl.multiple_of(q * rows, rows), rows)]

    def z_copies(g, s, way):
        two, one = groups[g]
        j = shard(s - 1, way)
        refs = [part(b, j, y) for b in two] + [b.at[j] for b in one]
        where = {"sp": z_next if way == 0 else z_prev}
        return [
            pltpu.make_async_remote_copy(
                src_ref=r, dst_ref=r, send_sem=zs.at[zbase[g] + k, way, s],
                recv_sem=zr.at[zbase[g] + k, way, s], device_id=where, device_id_type=MESH)
            for k, r in enumerate(refs)
        ]

    def z_arrivals(g, s, way):
        two, one = groups[g]
        j = shard(s, way)
        refs = [part(b, j, y) for b in two] + [b.at[j] for b in one]
        where = {"sp": z_next if way == 0 else z_prev}
        return [
            pltpu.make_async_remote_copy(
                src_ref=r, dst_ref=r, send_sem=zs.at[zbase[g] + k, way, s],
                recv_sem=zr.at[zbase[g] + k, way, s], device_id=where, device_id_type=MESH)
            for k, r in enumerate(refs)
        ]

    def y_copy(g, s, way, kind, q):
        j = shard(s, way)
        up = kind == 0 or (kind == 2 and way == 0)
        r = part(groups[g][0][0], j, q)
        return pltpu.make_async_remote_copy(
            src_ref=r, dst_ref=r, send_sem=ys.at[ybase[g], way, kind, s],
            recv_sem=yr.at[ybase[g], way, kind, s],
            device_id={"fs": y_next if up else y_prev}, device_id_type=MESH)

    y_far = lax.rem(y + 2, 4)

    def start_step(g, s, way):
        for c in z_copies(g, s, way):
            c.start()

    def comm(g, s):
        lasts = (n_right, n_left)
        for way in (0, 1):
            last = lasts[way]

            @pl.when((s >= 1) & (s <= last))
            def _():
                for c in z_arrivals(g, s, way):
                    c.wait_recv()

            @pl.when(s < last)
            def _():
                start_step(g, s + 1, way)

            if groups[g][0]:
                @pl.when((s >= 1) & (s <= last))
                def _():
                    y_copy(g, s, way, 0, y).start()
                    y_copy(g, s, way, 1, y).start()

                @pl.when((s >= 2) & (s <= last + 1))
                def _():
                    y_copy(g, s - 1, way, 0, y_prev).wait_recv()
                    y_copy(g, s - 1, way, 1, y_next).wait_recv()
                    y_copy(g, s - 1, way, 2, y_prev if way == 0 else y_next).start()

                @pl.when((s >= 3) & (s <= last + 2))
                def _():
                    y_copy(g, s - 2, way, 2, y_far).wait_recv()
                    y_copy(g, s - 2, way, 0, y).wait_send()
                    y_copy(g, s - 2, way, 1, y).wait_send()
                    y_copy(g, s - 2, way, 2, y_prev if way == 0 else y_next).wait_send()

            @pl.when((s >= 3) & (s <= last + 2))
            def _():
                for c in z_copies(g, s - 2, way):
                    c.wait_send()

    def both(ref, j1, j2, axis):
        return jnp.concatenate([ref[j1], ref[j2]], axis=axis)

    def multiply(g, s):
        if g == 3:
            return
        lag = s - 2
        j1 = jnp.where(lag == n_right, z, shard(lag, 0))
        j2 = shard(lag, 1)
        rows = both(normed, j1, j2, 1)
        if g == 0:
            w = jnp.concatenate([both(ap, j1, j2, 0), both(aq, j1, j2, 0)], axis=1)
            acc_a[...] += jnp.dot(rows, w, preferred_element_type=jnp.float32)
            acc_s[...] += lax.dot_general(
                rows, both(as_, j1, j2, 1), (((1,), (1,)), ((), ())),
                preferred_element_type=jnp.float32)
        elif g == 1:
            w = jnp.concatenate([both(bp, j1, j2, 0), both(bq, j1, j2, 0)], axis=1)
            acc_b[...] += jnp.dot(rows, w, preferred_element_type=jnp.float32)
        else:
            acc_c[...] += jnp.dot(rows, both(cp, j1, j2, 0), preferred_element_type=jnp.float32)

    for g in range(4):
        if offsets[g] == 0:
            start_step(g, 1, 0)
            start_step(g, 1, 1)

    def norm_rows(i, carry):
        at = pl.ds(pl.multiple_of(i * 32, 32), 32)
        x = tok[0, at, :].astype(jnp.float32)
        scale = lax.rsqrt(jnp.mean(x * x, axis=-1, keepdims=True) + 1e-06)
        x = (x * scale * gain[...]).astype(jnp.bfloat16)
        for j in range(n):
            normed[j, at, :] = x[:, j * 128:(j + 1) * 128]
        return carry

    lax.fori_loop(0, tok.shape[1] // 32, norm_rows, 0)
    for acc in (acc_a, acc_s, acc_b, acc_c):
        acc[...] = jnp.zeros_like(acc)

    def slot(t, carry):
        for g in range(4):
            s = t - offsets[g]
            low = 1 if offsets[g] == 0 else 0

            @pl.when((s >= low) & (s <= n_right + 2))
            def _():
                comm(g, s)
        for g in range(3):
            s = t - offsets[g]

            @pl.when((s >= 3) & (s <= n_right + 2))
            def _():
                multiply(g, s)
        return carry

    lax.fori_loop(1, n_right + 3 + max(offsets), slot, 0)
    o_inp[...] = acc_a[:, :256].astype(jnp.bfloat16)
    o_wr[...] = acc_a[:, 256:].astype(jnp.bfloat16)
    o_step[...] = acc_s[...].astype(jnp.bfloat16)
    o_gate[...] = acc_b[:, :256].astype(jnp.bfloat16)
    o_rd[...] = acc_b[:, 256:].astype(jnp.bfloat16)
    value = acc_c[:, :256].astype(jnp.bfloat16).astype(jnp.float32)
    sig = acc_c[:, 256:].astype(jnp.bfloat16).astype(jnp.float32)
    o_glu[...] = (value * jax.nn.sigmoid(sig)).astype(jnp.bfloat16)


def gather_project(n, tokens, gain, wi, ww, wst, wg, wr, wv, wsg, us, uf):
    t = tokens.shape[1]
    f32, bf = jnp.float32, jnp.bfloat16
    ws = jnp.pad(wst.T, ((0, 16 - wst.shape[1]), (0, 0)))
    vm = pl.BlockSpec(memory_space=pltpu.VMEM)
    hb = pl.BlockSpec(memory_space=pl.ANY)
    out = lambda *s: jax.ShapeDtypeStruct(s, bf)
    dma = pltpu.SemaphoreType.DMA
    steps = n // 2 + 1
    return pl.pallas_call(
        partial(gather_project_kernel, n, (0, 1, 3, 5)),
        out_shape=(out(t, 256), out(t, 256), out(t, 128), out(t, 128), out(t, 16), out(t, 256),
                   out(n, 256, 128), out(n, 256, 128)),
        in_specs=[vm, vm] + [hb] * 9,
        out_specs=(vm,) * 8,
        scratch_shapes=[
            pltpu.VMEM((n, t, 128), bf),
            pltpu.VMEM((n, 128, 256), bf), pltpu.VMEM((n, 128, 128), bf), pltpu.VMEM((n, 16, 128), bf),
            pltpu.VMEM((n, 128, 256), bf), pltpu.VMEM((n, 128, 128), bf),
            pltpu.VMEM((n, 128, 512), bf),
            pltpu.VMEM((t, 384), f32), pltpu.VMEM((t, 16), f32), pltpu.VMEM((t, 384), f32),
            pltpu.VMEM((t, 512), f32),
            dma((9,)), dma((8, 2, steps)), dma((8, 2, steps)),
            dma((4, 2, 3, steps)), dma((4, 2, 3, steps)),
        ],
        compiler_params=pltpu.CompilerParams(
            collective_id=0, has_side_effects=True, vmem_limit_bytes=60 * 1024 * 1024),
        name="gather_project",
    )(tokens, gain.reshape(1, -1), wi, ww, ws, wg, wr, wv, wsg, us, uf)


def in_one_piece(arrays, axis, dim, along):
    widths = [a.shape[along] for a in arrays]
    both = jnp.concatenate(arrays, axis=along)
    result = lax.all_gather(both, axis, axis=dim, tiled=True)
    return tuple(jnp.split(result, [sum(widths[:k]) for k in range(1, len(widths))], axis=along))


def passed_along(array, axis, by):
    length = lax.axis_size(axis)
    pairs = [(i, i + by) for i in range(length) if 0 <= i + by < length]
    return lax.ppermute(array, axis, pairs)


def laid_out(parts, dim):
    dims = list(parts.shape[1:])
    dims[dim] *= parts.shape[0]
    return jnp.moveaxis(parts, 0, dim).reshape(dims)


def from_everyone(array, axis):
    copies = jnp.broadcast_to(array, (lax.axis_size(axis), *array.shape))
    return lax.all_to_all(copies, axis, split_axis=0, concat_axis=0, tiled=True)


def collect(array, axis, dim):
    return laid_out(from_everyone(array, axis), dim)


def over_copies(array, axis):
    return from_everyone(array, axis).sum(axis=0)


def together(arrays, axis):
    ends = [0]
    for a in arrays:
        ends.append(ends[-1] + a.size)
    subtotal = over_copies(jnp.concatenate([a.ravel() for a in arrays]), axis)
    return tuple((subtotal[b:e].reshape(a.shape) for a, b, e in zip(arrays, ends, ends[1:])))


def split_up(array, dim, length):
    before, after = (array.shape[:dim], array.shape[dim + 1 :])
    return jnp.moveaxis(array.reshape(*before, length, -1, *after), dim, 0)


def summed_on_arrival(array, axis, dim):
    length = lax.axis_size(axis)
    parts = lax.all_to_all(split_up(array, dim, length), axis, 0, 0, tiled=True)
    return jnp.sum(parts.astype(jnp.float32), axis=0)


def causal_filter(border, values, kernel):
    extended = jnp.concatenate([border, values], axis=0).astype(jnp.float32)
    weights = kernel.astype(jnp.float32)
    row_count = values.shape[0]
    result = jnp.zeros(values.shape, jnp.float32)
    for offset in range(kernel.shape[0]):
        result = result + weights[offset] * extended[offset : offset + row_count]
    return result


def block_step(direct_gain, memory, pieces):
    input_block, write_block, read_block, step_block, log_block = pieces
    head_count = input_block.shape[1]
    per_group = head_count // write_block.shape[1]
    running = jnp.cumsum(log_block, axis=0)
    write_heads = jnp.repeat(write_block, per_group, axis=1)
    read_heads = jnp.repeat(read_block, per_group, axis=1)
    scores = jnp.einsum("lhn,shn->hls", read_heads, write_heads)
    spread = running.T[:, :, None] - running.T[:, None, :]
    row_index = lax.broadcasted_iota(jnp.int32, spread.shape, 1)
    col_index = lax.broadcasted_iota(jnp.int32, spread.shape, 2)
    decays = jnp.exp(jnp.where(row_index >= col_index, spread, -jnp.inf))
    scaled_inputs = input_block * step_block[:, :, None]
    inside = jnp.einsum("hls,shp->lhp", scores * decays, scaled_inputs)
    carried = jnp.exp(running)[:, :, None] * jnp.einsum("lhn,hpn->lhp", read_heads, memory)
    output = inside + carried + direct_gain[None, :, None] * input_block
    to_end = jnp.exp(running[-1][None, :] - running)
    fresh_terms = jnp.einsum("lhp,lhn->hpn", scaled_inputs * to_end[:, :, None], write_heads)
    new_memory = jnp.exp(running[-1])[:, None, None] * memory + fresh_terms
    return (new_memory, output)


def per_device(
    tokens,
    input_gain,
    weight_gate,
    weight_input,
    weight_write,
    weight_read,
    weight_step,
    weight_value,
    weight_sigmoid,
    filter_input,
    filter_write,
    filter_read,
    step_bias,
    rate_log,
    skip_gain,
    output_gain,
    opening_state,
    decay_shift,
    depth_filter,
    channel_gain,
    unproject_state,
    unproject_filter,
):
    row_count = tokens.shape[1]
    (gate_values, input_values, write_values, read_values, step_values, glu_rows, full_state,
     full_filter) = gather_project(
        lax.axis_size("sp"), tokens, input_gain, weight_input, weight_write, weight_step,
        weight_gate, weight_read, weight_value, weight_sigmoid, unproject_state, unproject_filter)
    step_values = step_values[:, : rate_log.shape[0]]
    full_state = full_state.transpose(1, 0, 2).reshape(256, -1)
    full_filter = full_filter.transpose(1, 0, 2).reshape(256, -1)
    short_rim = filter_input.shape[0] - 1
    long_rim = depth_filter.shape[0] - 1
    borders = passed_along(
        (
            input_values[row_count - short_rim :],
            write_values[row_count - short_rim :],
            read_values[row_count - short_rim :],
            glu_rows[row_count - long_rim :],
        ),
        "sp",
        1,
    )
    mixed_input = jax.nn.silu(causal_filter(borders[0], input_values, filter_input)).astype(
        jnp.bfloat16
    )
    mixed_write = jax.nn.silu(causal_filter(borders[1], write_values, filter_write)).astype(
        jnp.bfloat16
    )
    mixed_read = jax.nn.silu(causal_filter(borders[2], read_values, filter_read)).astype(
        jnp.bfloat16
    )
    head_count = rate_log.shape[0]
    group_count = mixed_write.shape[1] // STATE
    step_sizes = jax.nn.softplus(step_values.astype(jnp.float32) + step_bias)
    log_rates = -step_sizes * jnp.exp(rate_log) + decay_shift[0].T
    inputs_float = mixed_input.astype(jnp.float32).reshape(row_count, head_count, HEAD_DIM)
    write_float = mixed_write.astype(jnp.float32).reshape(row_count, group_count, STATE)
    read_float = mixed_read.astype(jnp.float32).reshape(row_count, group_count, STATE)
    block_count = row_count // BLOCK
    blocked = tuple(
        (
            array.reshape((block_count, BLOCK) + array.shape[1:])
            for array in (inputs_float, write_float, read_float, step_sizes, log_rates)
        )
    )
    zero_memory = jnp.zeros((head_count, HEAD_DIM, STATE), jnp.float32)
    local_memory, outputs = lax.scan(partial(block_step, skip_gain), zero_memory, blocked)
    outputs = outputs.reshape(row_count, head_count, HEAD_DIM)
    running = jnp.cumsum(log_rates, axis=0)
    total_decay = running[-1]
    totals = collect(total_decay[None, :], "sp", 0)
    inclusive = jnp.cumsum(totals, axis=0)
    exclusive = inclusive - totals
    my_index = lax.axis_index("sp")
    before = lax.dynamic_slice_in_dim(exclusive, my_index, 1, 0)[0]
    piece = collect(local_memory[None].astype(jnp.bfloat16), "sp", 0).astype(jnp.float32)
    piece_rows = piece.shape[0]
    owners = jnp.arange(piece_rows, dtype=jnp.int32)
    weights = jnp.exp(
        jnp.where((owners < my_index)[:, None], before[None, :] - inclusive, -jnp.inf)
    )
    leading_memory = jnp.zeros_like(local_memory) + jnp.einsum("jh,jhpn->hpn", weights, piece)
    entering = opening_state[0] * jnp.exp(before)[:, None, None] + leading_memory
    read_heads = jnp.repeat(read_float, head_count // group_count, axis=1)
    outputs = outputs + jnp.exp(running)[:, :, None] * jnp.einsum(
        "lhn,hpn->lhp", read_heads, entering
    )
    gated = outputs.reshape(row_count, -1) * jax.nn.silu(gate_values.astype(jnp.float32))
    grouped = gated.reshape(row_count, group_count, -1)
    grouped = grouped * lax.rsqrt(jnp.mean(grouped * grouped, axis=-1, keepdims=True) + 1e-06)
    state_out = (grouped.reshape(row_count, -1) * output_gain).astype(jnp.bfloat16)
    filtered = causal_filter(borders[3], glu_rows, depth_filter)
    channel_sums = together((jnp.sum(filtered, axis=1), jnp.sum(filtered * filtered, axis=1)), "tp")
    mean_value = channel_sums[0] / CM
    mean_square = channel_sums[1] / CM
    variance = mean_square - mean_value * mean_value
    normal_rows = (
        (filtered - mean_value[:, None]) * lax.rsqrt(variance + 1e-05)[:, None] * channel_gain
    )
    filter_out = jax.nn.silu(normal_rows).astype(jnp.bfloat16)
    summed = summed_on_arrival(
        (
            jnp.dot(state_out, full_state, preferred_element_type=jnp.float32)
            + jnp.dot(filter_out, full_filter, preferred_element_type=jnp.float32)
        ).astype(jnp.bfloat16),
        "tp",
        0,
    )
    return summed.astype(jnp.bfloat16)[None]


def solution(mesh):
    in_specs = (
        P("fs", "sp", None),
        P(),
        P("sp", "tp"),
        P("sp", "tp"),
        P("sp", "tp"),
        P("sp", "tp"),
        P("sp", "tp"),
        P("sp", "tp"),
        P("sp", "tp"),
        P(None, "tp"),
        P(None, "tp"),
        P(None, "tp"),
        P("tp"),
        P("tp"),
        P("tp"),
        P("tp"),
        P("fs", "tp", None, None),
        P("fs", "tp", "sp"),
        P(None, "tp"),
        P("tp"),
        P("tp", "sp"),
        P("tp", "sp"),
    )
    out_specs = P("fs", ("sp", "tp"), None)
    return jax.shard_map(
        per_device, mesh=mesh, in_specs=in_specs, out_specs=out_specs, check_vma=False
    )
```

```python
from functools import partial

import jax
import jax.numpy as jnp
from jax import lax
from jax.experimental import pallas as pl
from jax.experimental.pallas import tpu as pltpu
from jax.sharding import PartitionSpec as P

MESH = pl.DeviceIdType.MESH
F32, BF16 = jnp.float32, jnp.bfloat16
CHANNELS = 2048
OFFSETS = (0, 1, 3, 5)
AFTER = 2


def mixer_kernel(
    n,
    tok, gain, wi, ww, ws, wg, wr, wv, wsg, us, uf,
    f_in, f_wr, f_rd, bias, rate, skip, out_gain, opening, shift, taps, ch_gain,
    out,
    normed, ap, aq, as_, bp, bq, cp, up, uq, acc_a, acc_s, acc_b, acc_c,
    halo_src, halo_dst, glu_src, glu_dst, ext4, ext31, x_ref, b_ref, c_ref, gate_ref,
    rows_ref, cols_ref, inside, filtered, stat, ebuf, tbuf, e_right, e_left, run, act,
    pbuf, d2d_src, d2d_dst, far_src, far_dst, rn_src, rn_dst, dn_src, dn_dst,
    local_sem, zs, zr, ys, yr, es, er, hs, hr, ss, sr, os_, or_,
):
    z = lax.axis_index("sp")
    y = lax.axis_index("fs")
    tp = lax.axis_index("tp")
    x, core = tp // 2, lax.rem(tp, 2)
    n_right, n_left = n // 2, (n - 1) // 2
    z_next, z_prev = lax.rem(z + 1, n), lax.rem(z + n - 1, n)
    y_next, y_prev = lax.rem(y + 1, 4), lax.rem(y + 3, 4)
    t_rows = tok.shape[1]

    pairs = [
        (wi, ap.at[z]), (ww, aq.at[z]), (ws, as_.at[z]), (wg, bp.at[z]), (wr, bq.at[z]),
        (wv, cp.at[z, :, pl.ds(0, 256)]), (wsg, cp.at[z, :, pl.ds(256, 256)]),
        (us, up.at[z]), (uf, uq.at[z]),
    ]
    own = [pltpu.make_async_copy(s, d, local_sem.at[k]) for k, (s, d) in enumerate(pairs)]
    for c in own:
        c.start()
    barrier = pltpu.get_barrier_semaphore()
    greet = [{"sp": z_next}, {"sp": z_prev}, {"fs": y_next}, {"fs": y_prev}]
    greet += [{"tp": lax.rem(tp + i, 8)} for i in range(1, 8)]
    for where in greet:
        pl.semaphore_signal(barrier, inc=1, device_id=where, device_id_type=MESH)
    for c in own:
        c.wait()
    pl.semaphore_wait(barrier, len(greet))

    def remote(src, dst, send, recv, where):
        return pltpu.make_async_remote_copy(
            src_ref=src, dst_ref=dst, send_sem=send, recv_sem=recv, device_id=where,
            device_id_type=MESH)

    groups = [((ap,), (aq, as_)), ((bp,), (bq,)), ((cp,), ()), ((up,), (uq,))]
    zbase, zi = [], 0
    for two, one in groups:
        zbase.append(zi)
        zi += len(two) + len(one)

    def shard(s, way):
        return lax.rem(z + n - s, n) if way == 0 else lax.rem(z + s, n)

    def part(buf, j, q):
        rows = buf.shape[1] // 4
        return buf.at[j, pl.ds(pl.multiple_of(q * rows, rows), rows)]

    def z_copies(g, s, way, j):
        two, one = groups[g]
        refs = [part(b, j, y) for b in two] + [b.at[j] for b in one]
        where = {"sp": z_next if way == 0 else z_prev}
        return [
            remote(r, r, zs.at[zbase[g] + k, way, s], zr.at[zbase[g] + k, way, s], where)
            for k, r in enumerate(refs)
        ]

    def y_copy(g, s, way, kind, q):
        up_way = kind == 0 or (kind == 2 and way == 0)
        r = part(groups[g][0][0], shard(s, way), q)
        return remote(r, r, ys.at[g, way, kind, s], yr.at[g, way, kind, s],
                      {"fs": y_next if up_way else y_prev})

    y_far = lax.rem(y + 2, 4)

    def start_step(g, s, way):
        for c in z_copies(g, s, way, shard(s - 1, way)):
            c.start()

    def comm(g, s):
        for way in (0, 1):
            last = (n_right, n_left)[way]

            @pl.when((s >= 1) & (s <= last))
            def _():
                for c in z_copies(g, s, way, shard(s, way)):
                    c.wait_recv()

            @pl.when(s < last)
            def _():
                start_step(g, s + 1, way)

            @pl.when((s >= 1) & (s <= last))
            def _():
                y_copy(g, s, way, 0, y).start()
                y_copy(g, s, way, 1, y).start()

            @pl.when((s >= 2) & (s <= last + 1))
            def _():
                y_copy(g, s - 1, way, 0, y_prev).wait_recv()
                y_copy(g, s - 1, way, 1, y_next).wait_recv()
                y_copy(g, s - 1, way, 2, y_prev if way == 0 else y_next).start()

            @pl.when((s >= 3) & (s <= last + 2))
            def _():
                y_copy(g, s - 2, way, 2, y_far).wait_recv()
                y_copy(g, s - 2, way, 0, y).wait_send()
                y_copy(g, s - 2, way, 1, y).wait_send()
                y_copy(g, s - 2, way, 2, y_prev if way == 0 else y_next).wait_send()
                for c in z_copies(g, s - 2, way, shard(s - 3, way)):
                    c.wait_send()

    def both(ref, j1, j2, axis):
        return jnp.concatenate([ref[j1], ref[j2]], axis=axis)

    def multiply(g, s):
        lag = s - 2
        j1 = jnp.where(lag == n_right, z, shard(lag, 0))
        j2 = shard(lag, 1)
        rows = both(normed, j1, j2, 1)
        if g == 0:
            w = jnp.concatenate([both(ap, j1, j2, 0), both(aq, j1, j2, 0)], axis=1)
            acc_a[...] += jnp.dot(rows, w, preferred_element_type=F32)
            acc_s[:, :16] += lax.dot_general(
                rows, both(as_, j1, j2, 1), (((1,), (1,)), ((), ())),
                preferred_element_type=F32)
        elif g == 1:
            w = jnp.concatenate([both(bp, j1, j2, 0), both(bq, j1, j2, 0)], axis=1)
            acc_b[...] += jnp.dot(rows, w, preferred_element_type=F32)
        else:
            acc_c[...] += jnp.dot(rows, both(cp, j1, j2, 0), preferred_element_type=F32)

    def border(k):
        src, dst = [
            (halo_src.at[:, pl.ds(0, 384)], halo_dst.at[:, pl.ds(0, 384)]),
            (halo_src.at[:, pl.ds(384, 128)], halo_dst.at[:, pl.ds(384, 128)]),
            (glu_src, glu_dst),
        ][k]
        return remote(src, dst, hs.at[k], hr.at[k], {"sp": z_next})

    def short_filter(lo, hi, kernel, target):
        weights = [kernel[k:k + 1, :].astype(F32) for k in range(4)]

        def strip(i, carry):
            block = ext4[pl.ds(pl.multiple_of(i * 64, 64), 72), lo:hi]
            total = weights[0] * pltpu.roll(block, 72 - 5, 0)[:64]
            for k in range(1, 4):
                total = total + weights[k] * pltpu.roll(block, 72 - 5 - k, 0)[:64]
            target[pl.ds(pl.multiple_of(i * 64, 64), 64), :] = (
                total * jax.nn.sigmoid(total)).astype(BF16)
            return carry

        lax.fori_loop(0, t_rows // 64, strip, 0)

    def take_border(k, lo, hi):
        border(k).wait_recv()
        rows = halo_dst[:, lo:hi].astype(F32)[8:]
        ext4[0:8, lo:hi] = jnp.where(z > 0, rows, 0.0)

    def finish_a():
        mapped = acc_a[...].astype(BF16)
        halo_src[:, 0:384] = mapped[t_rows - 16:]
        ext4[8:, 0:384] = mapped.astype(F32)
        border(0).start()

    def finish_b():
        mapped = acc_b[...].astype(BF16)
        halo_src[:, 384:512] = mapped[t_rows - 16:, 256:]
        ext4[8:, 384:512] = mapped[:, 256:].astype(F32)
        border(1).start()
        gate_ref[...] = mapped[:, :256]

    def finish_c():
        value = acc_c[:, :256].astype(BF16).astype(F32)
        sig = acc_c[:, 256:].astype(BF16).astype(F32)
        glu = (value * jax.nn.sigmoid(sig)).astype(BF16)
        glu_src[...] = glu[t_rows - 32:]
        border(2).start()
        ext31[32:, :] = glu.astype(F32)

    lane = lax.broadcasted_iota(jnp.int32, (1, 128), 1)

    def by_head(first, rows=slice(None)):
        c = cols_ref[rows, first:first + 4]
        return jnp.concatenate(
            [jnp.where(lane < 64, c[:, 2 * k:2 * k + 1], c[:, 2 * k + 1:2 * k + 2])
             for k in range(2)], axis=1)

    def local_state():
        take_border(0, 0, 384)
        short_filter(0, 256, f_in, x_ref)
        short_filter(256, 384, f_wr, b_ref)
        head = lax.broadcasted_iota(jnp.int32, (8, t_rows), 0)
        place = lax.broadcasted_iota(jnp.int32, (8, t_rows), 1)
        bias8 = jnp.zeros((8, t_rows), F32)
        rate8 = jnp.zeros((8, t_rows), F32)
        for h in range(4):
            bias8 = jnp.where(head == h, bias[h], bias8)
            rate8 = jnp.where(head == h, rate[h], rate8)
        steps = acc_s[...].astype(BF16).astype(F32).T[:8] + bias8
        steps = jnp.maximum(steps, 0.0) + jnp.log1p(jnp.exp(-jnp.abs(steps)))
        rows_ref[0:4, :] = shift[0]
        rows_ref[4:8, :] = jnp.zeros((4, t_rows), F32)
        total = rows_ref[0:8, :] - steps * jnp.exp(rate8)
        k = 1
        while k < t_rows:
            total = total + jnp.where(place >= k, pltpu.roll(total, k, 1), 0.0)
            k *= 2
        end = total[:, t_rows - 1:t_rows]
        rows_ref[0:8, :] = total
        rows_ref[8:16, :] = steps
        rows_ref[16:24, :] = steps * jnp.exp(end - total)
        rows_ref[24:32, :] = jnp.exp(total)
        rows_ref[32:, :] = jnp.zeros((96, t_rows), F32)
        cols_ref[...] = rows_ref[...].T
        scaled = (x_ref[...].astype(F32) * by_head(16)).astype(BF16)
        ebuf[z] = lax.dot_general(
            b_ref[...], scaled, (((0,), (0,)), ((), ())), preferred_element_type=F32
        ).astype(BF16)
        spread = jnp.concatenate(
            [jnp.where(lane < 64, end[2 * k:2 * k + 1, :], end[2 * k + 1:2 * k + 2, :])
             for k in range(2)], axis=1)
        tbuf[z] = jnp.broadcast_to(spread, (8, 256))
        e_right[...] = jnp.zeros_like(e_right)
        run[...] = jnp.zeros_like(run)
        e_left[...] = opening[0].reshape(256, 128).T

    def e_copies(s, way, j):
        where = {"sp": z_next if way == 0 else z_prev}
        return [remote(r.at[j], r.at[j], es.at[k, way, s], er.at[k, way, s], where)
                for k, r in enumerate((ebuf, tbuf))]

    def state_ring(s):
        for way in (0, 1):
            last = (n_right, n_left)[way]

            @pl.when((s >= 1) & (s <= last))
            def _():
                for c in e_copies(s, way, shard(s, way)):
                    c.wait_recv()

            @pl.when(s < last)
            def _():
                for c in e_copies(s + 1, way, shard(s, way)):
                    c.start()

            @pl.when((s >= 1) & (s <= last))
            def _():
                for c in e_copies(s, way, shard(s - 1, way)):
                    c.wait_send()
                j = shard(s, way)
                total = tbuf[j][0:1]
                if way == 0:
                    @pl.when(z >= s)
                    def _():
                        e_right[...] += jnp.exp(run[0:1, :]) * ebuf[j].astype(F32)
                        run[...] += total
                else:
                    @pl.when(z + s >= n)
                    def _():
                        e_left[...] = e_left[...] * jnp.exp(total) + ebuf[j].astype(F32)

    def inside_strip(i):
        k = 128 * (i + 1)
        at = slice(128 * i, k)
        scores = lax.dot_general(
            c_ref[at, :], b_ref[0:k, :], (((1,), (1,)), ((), ())), preferred_element_type=F32)
        diag = (lax.broadcasted_iota(jnp.int32, (128, k), 0) + 128 * i
                >= lax.broadcasted_iota(jnp.int32, (128, k), 1))
        pieces = []
        for h in range(4):
            gap = cols_ref[at, h:h + 1] - rows_ref[h:h + 1, 0:k]
            decay = jnp.exp(jnp.where(diag, gap, -jnp.inf)) * rows_ref[8 + h:9 + h, 0:k]
            tile = slice(128 * (h // 2), 128 * (h // 2) + 128)
            pieces.append(jnp.dot((scores * decay).astype(BF16), x_ref[0:k, tile],
                                  preferred_element_type=F32))
        for k in range(2):
            gains = jnp.where(lane < 64, skip[2 * k], skip[2 * k + 1])
            lanes = slice(128 * k, 128 * k + 128)
            inside[at, lanes] = (jnp.where(lane < 64, pieces[2 * k], pieces[2 * k + 1])
                                 + gains * x_ref[at, lanes].astype(F32))

    def stat_copy(i, to):
        slot = tp if to else lax.rem(tp + 8 - i, 8)
        return remote(stat.at[slot], stat.at[slot], ss.at[i], sr.at[i],
                      {"tp": lax.rem(tp + i, 8)})

    def long_filter():
        border(2).wait_recv()
        ext31[0:32, :] = jnp.where(z > 0, glu_dst[...].astype(F32), 0.0)

        def strip(i, carry):
            block = ext31[pl.ds(pl.multiple_of(i * 32, 32), 64), :]
            total = jnp.zeros((32, 256), F32)
            for r in range(8):
                moved = block if r == 0 else pltpu.roll(block, 64 - r, 0)
                for a in range(5):
                    k = 8 * a + r - 2
                    if 0 <= k < 31 and 8 * a + 32 <= 64:
                        total = total + taps[k:k + 1, :].astype(F32) * moved[8 * a:8 * a + 32]
            at = pl.ds(pl.multiple_of(i * 32, 32), 32)
            filtered[at, :] = total
            inside_sums = jnp.concatenate(
                [jnp.sum(total, axis=1, keepdims=True),
                 jnp.sum(total * total, axis=1, keepdims=True)], axis=1)
            cols_ref[at, 64:66] = inside_sums
            return carry

        lax.fori_loop(0, t_rows // 32, strip, 0)
        stat[tp] = cols_ref[...].T[64:72]
        for i in range(1, 8):
            stat_copy(i, True).start()

    def filter_act():
        for i in range(1, 8):
            stat_copy(i, False).wait_recv()
        sums = stat[0]
        for i in range(1, 8):
            sums = sums + stat[i]
        mean = sums[0:1] / CHANNELS
        var = sums[1:2] / CHANNELS - mean * mean
        scale = lax.rsqrt(var + 1e-05)
        rows_ref[32:33, :] = mean
        rows_ref[33:34, :] = scale
        back = rows_ref[...].T

        def strip(i, carry):
            at = pl.ds(pl.multiple_of(i * 64, 64), 64)
            f = (filtered[at, :] - cols_ref[at, 32:33]) * cols_ref[at, 33:34] * ch_gain[...]
            act[at, 256:512] = (f * jax.nn.sigmoid(f)).astype(BF16)
            return carry

        cols_ref[:, 32:34] = back[:, 32:34]
        lax.fori_loop(0, t_rows // 64, strip, 0)
        for i in range(1, 8):
            stat_copy(i, True).wait_send()

    for g in range(4):
        if OFFSETS[g] == 0:
            start_step(g, 1, 0)
            start_step(g, 1, 1)

    def norm_rows(i, carry):
        at = pl.ds(pl.multiple_of(i * 32, 32), 32)
        v = tok[0, at, :].astype(F32)
        scale = lax.rsqrt(jnp.mean(v * v, axis=-1, keepdims=True) + 1e-06)
        v = (v * scale * gain[...]).astype(BF16)
        for j in range(n):
            normed[j, at, :] = v[:, j * 128:(j + 1) * 128]
        return carry

    lax.fori_loop(0, t_rows // 32, norm_rows, 0)
    for acc in (acc_a, acc_s, acc_b, acc_c):
        acc[...] = jnp.zeros_like(acc)

    done = [n_right + 2 + o for o in OFFSETS]
    state_at = done[0] + AFTER
    read_at = max(done[1] + AFTER, state_at + 1)
    long_at = done[2] + AFTER
    last_slot = max(max(done), state_at + n_right, read_at + 4, long_at + 4) + 1

    def slot(t, carry):
        for g in range(4):
            s = t - OFFSETS[g]
            low = 1 if OFFSETS[g] == 0 else 0

            @pl.when((s >= low) & (s <= n_right + 2))
            def _():
                comm(g, s)

        @pl.when((t > state_at) & (t <= state_at + n_right))
        def _():
            state_ring(t - state_at)

        for g in range(3):
            s = t - OFFSETS[g]

            @pl.when((s >= 3) & (s <= n_right + 2))
            def _():
                multiply(g, s)

        @pl.when(t == done[0])
        def _():
            finish_a()

        @pl.when(t == done[1])
        def _():
            finish_b()

        @pl.when(t == done[2])
        def _():
            finish_c()

        @pl.when(t == state_at)
        def _():
            local_state()
            for way in (0, 1):
                for c in e_copies(1, way, z):
                    c.start()

        @pl.when(t == long_at)
        def _():
            long_filter()

        @pl.when(t == read_at)
        def _():
            take_border(1, 384, 512)
            short_filter(384, 512, f_rd, c_ref)

        for i in range(4):
            @pl.when(t == read_at + 1 + i)
            def _():
                inside_strip(i)

        @pl.when(t == long_at + 3)
        def _():
            filter_act()
        return carry

    lax.fori_loop(1, last_slot, slot, 0)
    for k in range(3):
        border(k).wait_send()

    entering = (e_left[...] * jnp.exp(run[0:1, :]) + e_right[...]).astype(BF16)
    for i in range(4):
        at = slice(128 * i, 128 * i + 128)
        carried = jnp.dot(c_ref[at, :], entering, preferred_element_type=F32)
        v = inside[at, :] + by_head(24, at) * carried
        g = gate_ref[at, :].astype(F32)
        v = v * (g * jax.nn.sigmoid(g))
        v = v * lax.rsqrt(jnp.mean(v * v, axis=-1, keepdims=True) + 1e-06)
        act[at, 0:256] = (v * out_gain[...]).astype(BF16)

    blocks = CHANNELS // 256

    def rows_of(xx, cc):
        return pl.ds(pl.multiple_of((2 * xx + cc) * 64, 64), 64)

    def at_x(k):
        return {"tp": 2 * lax.rem(x + k, 4) + core}

    def pair_copy(b):
        return remote(d2d_src.at[b], d2d_dst.at[b], os_.at[0, b], or_.at[0, b],
                      {"tp": 2 * x + 1 - core})

    def far_copy(b):
        return remote(far_src.at[b], far_dst.at[b], os_.at[1, b], or_.at[1, b],
                      at_x(1 + 2 * lax.rem(b, 2)))

    def relay_copy(b):
        return remote(rn_src.at[b], rn_dst.at[b], os_.at[2, b], or_.at[2, b],
                      at_x(1 + 2 * lax.rem(b, 2)))

    def direct_copy(b):
        return remote(dn_src.at[b], dn_dst.at[b], os_.at[3, b], or_.at[3, b],
                      at_x(3 + 2 * lax.rem(b, 2)))

    def stage_multiply(b):
        w = jnp.concatenate(
            [jnp.concatenate([ref[2 * b], ref[2 * b + 1]], axis=1) for ref in (up, uq)], axis=0)
        pbuf[b] = jnp.dot(act[...], w, preferred_element_type=F32)
        for xx in range(4):
            d2d_src[b, xx] = pbuf[b, rows_of(xx, 1 - core), :].astype(BF16)
        pair_copy(b).start()

    def stage_pair(b):
        pair_copy(b).wait_recv()
        for xx in range(4):
            at = rows_of(xx, core)
            pbuf[b, at, :] = pbuf[b, at, :] + d2d_dst[b, xx].astype(F32)
        far_src[b] = pbuf[b, rows_of(lax.rem(x + 2, 4), core), :].astype(BF16)
        far_copy(b).start()
        dn_src[b] = pbuf[b, rows_of(lax.rem(x + 3 + 2 * lax.rem(b, 2), 4), core), :].astype(BF16)
        direct_copy(b).start()

    def stage_relay(b):
        far_copy(b).wait_recv()
        mine = pbuf[b, rows_of(lax.rem(x + 1 + 2 * lax.rem(b, 2), 4), core), :]
        rn_src[b] = (mine + far_dst[b].astype(F32)).astype(BF16)
        relay_copy(b).start()

    def stage_out(b):
        relay_copy(b).wait_recv()
        direct_copy(b).wait_recv()
        total = (pbuf[b, rows_of(x, core), :] + rn_dst[b].astype(F32)) + dn_dst[b].astype(F32)
        out[0, :, pl.ds(pl.multiple_of(b * 256, 256), 256)] = total.astype(BF16)
        for c in (pair_copy(b), far_copy(b), relay_copy(b), direct_copy(b)):
            c.wait_send()

    def out_slot(i, carry):
        @pl.when(i < blocks)
        def _():
            stage_multiply(i)

        for lag, stage in ((2, stage_pair), (5, stage_relay), (8, stage_out)):
            @pl.when((i >= lag) & (i < blocks + lag))
            def _():
                stage(i - lag)
        return carry

    lax.fori_loop(0, blocks + 8, out_slot, 0)


def per_device(
    tokens, input_gain, weight_gate, weight_input, weight_write, weight_read, weight_step,
    weight_value, weight_sigmoid, filter_input, filter_write, filter_read, step_bias, rate_log,
    skip_gain, output_gain, opening_state, decay_shift, depth_filter, channel_gain,
    unproject_state, unproject_filter,
):
    n = lax.axis_size("sp")
    t = tokens.shape[1]
    ws = jnp.pad(weight_step.T, ((0, 16 - weight_step.shape[1]), (0, 0)))
    vm = pl.BlockSpec(memory_space=pltpu.VMEM)
    sm = pl.BlockSpec(memory_space=pltpu.SMEM)
    hb = pl.BlockSpec(memory_space=pl.ANY)
    dma = pltpu.SemaphoreType.DMA
    steps = n // 2 + 1
    v = pltpu.VMEM
    return pl.pallas_call(
        partial(mixer_kernel, n),
        out_shape=jax.ShapeDtypeStruct((1, t // 8, CHANNELS), BF16),
        in_specs=[vm, vm] + [hb] * 9 + [vm] * 3 + [sm] * 3 + [vm] * 5,
        out_specs=vm,
        scratch_shapes=[
            v((n, t, 128), BF16),
            v((n, 128, 256), BF16), v((n, 128, 128), BF16), v((n, 16, 128), BF16),
            v((n, 128, 256), BF16), v((n, 128, 128), BF16), v((n, 128, 512), BF16),
            v((n, 256, 128), BF16), v((n, 256, 128), BF16),
            v((t, 384), F32), v((t, 128), F32), v((t, 384), F32), v((t, 512), F32),
            v((16, 512), BF16), v((16, 512), BF16), v((32, 256), BF16), v((32, 256), BF16),
            v((8 + t, 512), F32), v((32 + t, 256), F32),
            v((t, 256), BF16), v((t, 128), BF16), v((t, 128), BF16), v((t, 256), BF16),
            v((128, t), F32), v((t, 128), F32), v((t, 256), F32), v((t, 256), F32),
            v((8, 8, t), F32), v((n, 128, 256), BF16), v((n, 8, 256), F32),
            v((128, 256), F32), v((128, 256), F32), v((8, 256), F32), v((t, 512), BF16),
            v((8, t, 256), F32), v((8, 4, 64, 256), BF16), v((8, 4, 64, 256), BF16),
            *[v((8, 64, 256), BF16)] * 6,
            dma((9,)), dma((8, 2, steps)), dma((8, 2, steps)),
            dma((4, 2, 3, steps)), dma((4, 2, 3, steps)),
            dma((2, 2, steps)), dma((2, 2, steps)), dma((3,)), dma((3,)),
            dma((8,)), dma((8,)), dma((4, 8)), dma((4, 8)),
        ],
        compiler_params=pltpu.CompilerParams(
            collective_id=0, has_side_effects=True, vmem_limit_bytes=62 * 1024 * 1024),
        name="mixer",
    )(
        tokens, input_gain.reshape(1, -1), weight_input, weight_write, ws, weight_gate,
        weight_read, weight_value, weight_sigmoid, unproject_state, unproject_filter,
        filter_input, filter_write, filter_read, step_bias, rate_log, skip_gain,
        output_gain.reshape(1, -1), opening_state, decay_shift, depth_filter,
        channel_gain.reshape(1, -1),
    )


def solution(mesh):
    in_specs = (
        P("fs", "sp", None),
        P(),
        P("sp", "tp"),
        P("sp", "tp"),
        P("sp", "tp"),
        P("sp", "tp"),
        P("sp", "tp"),
        P("sp", "tp"),
        P("sp", "tp"),
        P(None, "tp"),
        P(None, "tp"),
        P(None, "tp"),
        P("tp"),
        P("tp"),
        P("tp"),
        P("tp"),
        P("fs", "tp", None, None),
        P("fs", "tp", "sp"),
        P(None, "tp"),
        P("tp"),
        P("tp", "sp"),
        P("tp", "sp"),
    )
    out_specs = P("fs", ("sp", "tp"), None)
    return jax.shard_map(
        per_device, mesh=mesh, in_specs=in_specs, out_specs=out_specs, check_vma=False
    )
```

```python
from functools import partial

import jax
import jax.numpy as jnp
from jax import lax
from jax.experimental import pallas as pl
from jax.experimental.pallas import tpu as pltpu
from jax.sharding import PartitionSpec as P

MESH = pl.DeviceIdType.MESH
F32, BF16 = jnp.float32, jnp.bfloat16
CHANNELS = 2048
OFFSETS = (0, 1, 8)
LONG_TO_ACT = 3


def mixer_kernel(
    n,
    tok_h, gain_h, wi, ww, ws_h, wg, wr, wv, wsg, us, uf,
    f_in_h, f_wr_h, f_rd_h, bias_h, rate_h, skip_h, out_gain_h, opening_h, shift_h, taps_h,
    ch_gain_h,
    out,
    tok, gain, ws_v, f_in, f_wr, f_rd, bias, rate, skip, out_gain, opening, shift, taps, ch_gain,
    normed, ap, aq, as_, cp, cq, up, acc_a, acc_s, acc_c, blank, tapsb,
    tok_edge, ext4, ext31, x_ref, b_ref, c_ref, gate_ref,
    rows_ref, cols_ref, inside, filtered, sums_ref, stat, ebuf, tbuf, e_right, e_left, run, act,
    pbuf, d2d_src, d2d_dst, far_src, far_dst, rn_src, rn_dst, dn_src, dn_dst,
    local_sem, zs, zr, ys, yr, es, er, hs, hr, ss, sr, os_, or_,
):
    z = lax.axis_index("sp")
    y = lax.axis_index("fs")
    tp = lax.axis_index("tp")
    x, core = tp // 2, lax.rem(tp, 2)
    n_right, n_left = n // 2, (n - 1) // 2
    z_next, z_prev = lax.rem(z + 1, n), lax.rem(z + n - 1, n)
    y_next, y_prev = lax.rem(y + 1, 4), lax.rem(y + 3, 4)
    t_rows = tok.shape[0]

    barrier = pltpu.get_barrier_semaphore()
    greet = [{"sp": z_next}, {"sp": z_prev}, {"fs": y_next}, {"fs": y_prev}]
    greet += [{"tp": lax.rem(tp + i, 8)} for i in range(1, 8)]
    for where in greet:
        pl.semaphore_signal(barrier, inc=1, device_id=where, device_id_type=MESH)

    pairs = [
        (ws_h, ws_v), (wi, ap.at[z, :, pl.ds(0, 256)]), (wg, ap.at[z, :, pl.ds(256, 256)]),
        (ww, aq.at[z, :, pl.ds(0, 128)]), (wr, aq.at[z, :, pl.ds(128, 128)]),
        (tok_h.at[0], tok), (gain_h, gain), (wv, cp.at[z, :, pl.ds(0, 256)]),
        (wsg.at[:, pl.ds(0, 128)], cp.at[z, :, pl.ds(256, 128)]),
        (wsg.at[:, pl.ds(128, 128)], cq.at[z]),
        (us, up.at[z, pl.ds(0, 256)]), (uf, up.at[z, pl.ds(256, 256)]),
        (f_in_h, f_in), (f_wr_h, f_wr), (f_rd_h, f_rd), (bias_h, bias), (rate_h, rate),
        (skip_h, skip), (out_gain_h, out_gain), (opening_h.at[0], opening),
        (shift_h.at[0], shift), (taps_h, taps), (ch_gain_h, ch_gain),
    ]
    own = [pltpu.make_async_copy(s, d, local_sem.at[k]) for k, (s, d) in enumerate(pairs)]
    for c in own:
        c.start()

    def remote(src, dst, send, recv, where):
        return pltpu.make_async_remote_copy(
            src_ref=src, dst_ref=dst, send_sem=send, recv_sem=recv, device_id=where,
            device_id_type=MESH)

    def wait_bytes(sem, count):
        ref = blank.at[pl.ds(0, count // 512)]
        pltpu.make_async_copy(ref, ref, sem).wait()

    groups = [(ap, (aq, as_)), (cp, (cq,)), (up, ())]
    part_bytes = [ref.shape[1] // 4 * ref.shape[2] * 2 for ref, _ in groups]
    z_bytes = [p + sum(ref.shape[1] * ref.shape[2] * 2 for ref in one)
               for p, (_, one) in zip(part_bytes, groups)]

    def shard(s, way):
        return lax.rem(z + n - s, n) if way == 0 else lax.rem(z + s, n)

    def part(buf, j, q):
        rows = buf.shape[1] // 4
        return buf.at[j, pl.ds(pl.multiple_of(q * rows, rows), rows)]

    def pieces(g, c, j):
        two, one = groups[g]
        if c == 0:
            return [part(two, j, y)]
        rows = one[0].shape[1] // 2
        more = [b.at[j] for b in one[1:]] if c == 2 else []
        return [one[0].at[j, pl.ds((c - 1) * rows, rows)]] + more

    chunks = [3 if one else 1 for _, one in groups]
    first = [sum(chunks[:g]) for g in range(len(groups))]

    def chunk_bytes(g, c):
        if c == 0:
            return part_bytes[g]
        one = groups[g][1]
        rest = sum(r.shape[1] * r.shape[2] * 2 for r in one[1:]) if c == 2 else 0
        return one[0].shape[1] * one[0].shape[2] + rest

    def start_chunk(g, c, s, way):
        for r in pieces(g, c, shard(s - 1, way)):
            remote(r, r, zs.at[g, way, lax.rem(s, 4)], zr.at[first[g] + c, way, s - 1],
                   {"sp": z_next if way == 0 else z_prev}).start()

    y_far = lax.rem(y + 2, 4)
    direct_from = n_right - 1

    def y_start(g, s, way, kind, q):
        up_way = kind == 0 or (kind == 2 and way == 0)
        r = part(groups[g][0], shard(s, way), q)
        k = kind // 2
        where = y_far if kind == 3 else (y_next if up_way else y_prev)
        remote(r, r, ys.at[g, k, lax.rem(s, 4)], yr.at[g, k, s - 1], {"fs": where}).start()

    def y_wait(sem, g, s, per_way):
        @pl.when(s <= n_left)
        def _():
            wait_bytes(sem, 2 * per_way * part_bytes[g])

        @pl.when(s > n_left)
        def _():
            wait_bytes(sem, per_way * part_bytes[g])

    def comm(g, s):
        for c in range(chunks[g]):
            for way in (0, 1):
                last = (n_right, n_left)[way]

                @pl.when((s >= 1) & (s <= last))
                def _():
                    wait_bytes(zr.at[first[g] + c, way, s - 1], chunk_bytes(g, c))

                @pl.when(s < last)
                def _():
                    start_chunk(g, c, s + 1, way)

                if c == 0:
                    @pl.when((s >= 1) & (s <= last))
                    def _():
                        y_start(g, s, way, 0, y)
                        y_start(g, s, way, 1, y)

                        @pl.when(s >= direct_from)
                        def _():
                            y_start(g, s, way, 3, y)

        @pl.when((s >= 3) & (s <= n_right + 2))
        def _():
            wait_bytes(zs.at[g, 0, lax.rem(s - 2, 4)], z_bytes[g])

            @pl.when(s - 2 <= n_left)
            def _():
                wait_bytes(zs.at[g, 1, lax.rem(s - 2, 4)], z_bytes[g])

    def share(g, s):
        @pl.when((s >= 2) & (s <= n_right + 1))
        def _():
            y_wait(yr.at[g, 0, s - 2], g, s - 1, 2)

            @pl.when(s - 1 < direct_from)
            def _():
                y_start(g, s - 1, 0, 2, y_prev)
                y_start(g, s - 1, 1, 2, y_next)

        def complete(k, carry):
            y_wait(yr.at[g, 1, k - 1], g, k, 1)
            y_wait(ys.at[g, 0, lax.rem(k, 4)], g, k, 2)
            y_wait(ys.at[g, 1, lax.rem(k, 4)], g, k, 1)
            if g < 2:
                with jax.named_scope("mm"):
                    multiply(g, k)
            return carry

        @pl.when((s >= 4) & (s <= n_right + 2))
        def _():
            low = jnp.where(s > n_right + 1, s - 2, s - 3)
            high = jnp.where(s > n_right, s - 2, s - 3)
            lax.fori_loop(low, high + 1, complete, 0)

    def both(ref, j1, j2, axis):
        return jnp.concatenate([ref[j1], ref[j2]], axis=axis)

    def multiply(g, k):
        j1 = jnp.where(k == n_right, z, shard(k, 0))
        j2 = shard(k, 1)
        rows = both(normed, j1, j2, 1)
        if g == 0:
            w = jnp.concatenate([both(ap, j1, j2, 0), both(aq, j1, j2, 0)], axis=1)
            acc_a[...] += jnp.dot(rows, w, preferred_element_type=F32)
            acc_s[:, :16] += lax.dot_general(
                rows, both(as_, j1, j2, 1), (((1,), (1,)), ((), ())),
                preferred_element_type=F32)
        else:
            w = jnp.concatenate([both(cp, j1, j2, 0), both(cq, j1, j2, 0)], axis=1)
            acc_c[...] += jnp.dot(rows, w, preferred_element_type=F32)

    edge_lanes = pl.ds(pl.multiple_of(tp * 256, 256), 256)

    def border():
        return remote(tok.at[pl.ds(t_rows - 32, 32), edge_lanes], tok_edge.at[:, edge_lanes],
                      hs.at[0], hr.at[0], {"sp": z_next})

    def border_share(i):
        ref = tok_edge.at[:, edge_lanes]
        return remote(ref, ref, hs.at[1], hr.at[1], {"tp": lax.rem(tp + i, 8)})

    def short_filter(lo, hi, kernel, target):
        weights = [kernel[k:k + 1, :].astype(F32) for k in range(4)]

        def strip(i, carry):
            block = ext4[pl.ds(pl.multiple_of(i * 64, 64), 72), lo:hi]
            total = weights[0] * pltpu.roll(block, 72 - 5, 0)[:64]
            for k in range(1, 4):
                total = total + weights[k] * pltpu.roll(block, 72 - 5 - k, 0)[:64]
            target[pl.ds(pl.multiple_of(i * 64, 64), 64), :] = (
                total * jax.nn.sigmoid(total)).astype(BF16)
            return carry

        lax.fori_loop(0, t_rows // 64, strip, 0)

    def finish_a():
        mapped = acc_a[...].astype(BF16)
        own_rows = mapped[:t_rows]
        edge = jnp.where(z > 0, acc_a[t_rows + 24:, :].astype(BF16).astype(F32), 0.0)
        ext4[0:8, 0:256] = edge[:, 0:256]
        ext4[0:8, 256:512] = edge[:, 512:768]
        ext4[8:, 0:256] = own_rows[:, 0:256].astype(F32)
        ext4[8:, 256:512] = own_rows[:, 512:768].astype(F32)
        gate_ref[...] = own_rows[:, 256:512]

    def finish_c():
        value = acc_c[:, :256].astype(BF16).astype(F32)
        sig = acc_c[:, 256:].astype(BF16).astype(F32)
        glu = (value * jax.nn.sigmoid(sig)).astype(BF16).astype(F32)
        ext31[0:32, :] = jnp.where(z > 0, glu[t_rows:], 0.0)
        ext31[32:, :] = glu[:t_rows]

    lane = lax.broadcasted_iota(jnp.int32, (1, 128), 1)

    def by_head(first, rows=slice(None)):
        c = cols_ref[rows, first:first + 4]
        return jnp.concatenate(
            [jnp.where(lane < 64, c[:, 2 * k:2 * k + 1], c[:, 2 * k + 1:2 * k + 2])
             for k in range(2)], axis=1)

    def local_state():
        short_filter(0, 256, f_in, x_ref)
        short_filter(256, 384, f_wr, b_ref)
        head = lax.broadcasted_iota(jnp.int32, (8, t_rows), 0)
        place = lax.broadcasted_iota(jnp.int32, (8, t_rows), 1)
        bias8 = jnp.zeros((8, t_rows), F32)
        rate8 = jnp.zeros((8, t_rows), F32)
        for h in range(4):
            bias8 = jnp.where(head == h, bias[h], bias8)
            rate8 = jnp.where(head == h, rate[h], rate8)
        steps = acc_s[0:t_rows, :].astype(BF16).astype(F32).T[:8] + bias8
        steps = jnp.maximum(steps, 0.0) + jnp.log1p(jnp.exp(-jnp.abs(steps)))
        rows_ref[0:4, :] = shift[...]
        rows_ref[4:8, :] = jnp.zeros((4, t_rows), F32)
        total = rows_ref[0:8, :] - steps * jnp.exp(rate8)
        k = 1
        while k < t_rows:
            total = total + jnp.where(place >= k, pltpu.roll(total, k, 1), 0.0)
            k *= 2
        end = total[:, t_rows - 1:t_rows]
        rows_ref[0:8, :] = total
        rows_ref[8:16, :] = steps
        rows_ref[16:24, :] = steps * jnp.exp(end - total)
        rows_ref[24:32, :] = jnp.exp(total)
        rows_ref[32:, :] = jnp.zeros((96, t_rows), F32)
        cols_ref[...] = rows_ref[...].T
        scaled = (x_ref[...].astype(F32) * by_head(16)).astype(BF16)
        ebuf[z] = lax.dot_general(
            b_ref[...], scaled, (((0,), (0,)), ((), ())), preferred_element_type=F32
        ).astype(BF16)
        spread = jnp.concatenate(
            [jnp.where(lane < 64, end[2 * k:2 * k + 1, :], end[2 * k + 1:2 * k + 2, :])
             for k in range(2)], axis=1)
        tbuf[z] = jnp.broadcast_to(spread, (8, 256))

    e_bytes = (2 * 32 * 256,) * 3 + (2 * 32 * 256 + 4 * 8 * 256,)

    def state_start(c, s, way):
        j = shard(s - 1, way)
        where = {"sp": z_next if way == 0 else z_prev}
        for r in [ebuf.at[j, pl.ds(32 * c, 32)]] + [tbuf.at[j]] * (c // 3):
            remote(r, r, es.at[way, lax.rem(s, 2)], er.at[c, way, s - 1], where).start()

    def state_ring(s):
        for c in range(4):
            for way in (0, 1):
                last = (n_right, n_left)[way]

                @pl.when(s <= last)
                def _():
                    wait_bytes(er.at[c, way, s - 1], e_bytes[c])

                @pl.when(s < last)
                def _():
                    state_start(c, s + 1, way)

        for way in (0, 1):
            last = (n_right, n_left)[way]

            @pl.when(s <= last)
            def _():
                j = shard(s, way)
                total = tbuf[j][0:1]
                if way == 0:
                    @pl.when(z >= s)
                    def _():
                        e_right[...] += jnp.exp(run[0:1, :]) * ebuf[j].astype(F32)
                        run[...] += total
                else:
                    @pl.when(z + s >= n)
                    def _():
                        e_left[...] = e_left[...] * jnp.exp(total) + ebuf[j].astype(F32)
                wait_bytes(es.at[way, lax.rem(s, 2)], sum(e_bytes))

    def inside_strip(i):
        k = 128 * (i + 1)
        at = slice(128 * i, k)
        scores = lax.dot_general(
            c_ref[at, :], b_ref[0:k, :], (((1,), (1,)), ((), ())), preferred_element_type=F32)
        diag = (lax.broadcasted_iota(jnp.int32, (128, k), 0) + 128 * i
                >= lax.broadcasted_iota(jnp.int32, (128, k), 1))
        pieces = []
        for h in range(4):
            gap = cols_ref[at, h:h + 1] - rows_ref[h:h + 1, 0:k]
            decay = jnp.exp(jnp.where(diag, gap, -jnp.inf)) * rows_ref[8 + h:9 + h, 0:k]
            tile = slice(128 * (h // 2), 128 * (h // 2) + 128)
            pieces.append(jnp.dot((scores * decay).astype(BF16), x_ref[0:k, tile],
                                  preferred_element_type=F32))
        for k in range(2):
            gains = jnp.where(lane < 64, skip[2 * k], skip[2 * k + 1])
            lanes = slice(128 * k, 128 * k + 128)
            inside[at, lanes] = (jnp.where(lane < 64, pieces[2 * k], pieces[2 * k + 1])
                                 + gains * x_ref[at, lanes].astype(F32))

    def stat_copy(i):
        return remote(stat.at[tp], stat.at[tp], ss.at[0], sr.at[0], {"tp": lax.rem(tp + i, 8)})

    def long_filter(half):
        def strip(i, carry):
            block = ext31[pl.ds(pl.multiple_of(i * 64, 64), 96), :]
            total = jnp.zeros((8, 8, 256), F32)
            for r in range(8):
                moved = block if r == 0 else pltpu.roll(block, 96 - r, 0)
                for a in range(5):
                    k = 8 * a + r - 2
                    if 0 <= k < 31:
                        total = total + (tapsb[8 * k:8 * k + 8, :][None]
                                         * moved[8 * a:8 * a + 64].reshape(8, 8, 256))
            total = total.reshape(64, 256)
            at = pl.ds(pl.multiple_of(i * 64, 64), 64)
            filtered[at, :] = total
            sum1 = jnp.sum(total, axis=1, keepdims=True)
            sum2 = jnp.sum(total * total, axis=1, keepdims=True)
            sums_ref[at, :] = jnp.where(lane == 0, sum1, jnp.where(lane == 1, sum2, 0.0))
            return carry

        lax.fori_loop(half * (t_rows // 128), (half + 1) * (t_rows // 128), strip, 0)

    def send_sums():
        stat[tp] = sums_ref[...].T[0:8]
        for i in range(1, 8):
            stat_copy(i).start()

    def filter_act():
        with jax.named_scope("fact_wait"):
            wait_bytes(sr.at[0], 7 * 8 * t_rows * 4)
        sums = stat[0]
        for i in range(1, 8):
            sums = sums + stat[i]
        mean = sums[0:1] / CHANNELS
        var = sums[1:2] / CHANNELS - mean * mean
        rows_ref[32:33, :] = mean
        rows_ref[33:34, :] = lax.rsqrt(var + 1e-05)
        sums_ref[...] = rows_ref[...].T

        def strip(i, carry):
            at = pl.ds(pl.multiple_of(i * 64, 64), 64)
            f = (filtered[at, :] - sums_ref[at, 32:33]) * sums_ref[at, 33:34] * ch_gain[...]
            act[at, 256:512] = (f * jax.nn.sigmoid(f)).astype(BF16)
            return carry

        lax.fori_loop(0, t_rows // 64, strip, 0)
        wait_bytes(ss.at[0], 7 * 8 * t_rows * 4)

    own[0].wait()
    as_[z] = jnp.concatenate([ws_v[...].astype(F32), jnp.zeros((12, 128), F32)]).astype(BF16)
    for c in own[1:5]:
        c.wait()
    with jax.named_scope("entry"):
        pl.semaphore_wait(barrier, len(greet))
    for c in range(chunks[0]):
        start_chunk(0, c, 1, 0)
        start_chunk(0, c, 1, 1)
    for c in own[5:]:
        c.wait()

    border().start()

    def norm_rows(source, at, to):
        v = source[at, :].astype(F32)
        scale = lax.rsqrt(jnp.mean(v * v, axis=-1, keepdims=True) + 1e-06)
        v = (v * scale * gain[...]).astype(BF16)
        for j in range(n):
            normed[j, to, :] = v[:, j * 128:(j + 1) * 128]

    def norm_strip(i, carry):
        at = pl.ds(pl.multiple_of(i * 32, 32), 32)
        norm_rows(tok, at, at)
        return carry

    with jax.named_scope("norm"):
        lax.fori_loop(0, t_rows // 32, norm_strip, 0)
    e_right[...] = jnp.zeros_like(e_right)
    run[...] = jnp.zeros_like(run)
    e_left[...] = opening[...].reshape(256, 128).T
    for acc in (acc_a, acc_s, acc_c):
        acc[...] = jnp.zeros_like(acc)
    for k in range(taps.shape[0]):
        tapsb[8 * k:8 * k + 8, :] = jnp.broadcast_to(
            taps[k:k + 1, :].astype(F32), (8, 256))

    done = [n_right + 2 + o for o in OFFSETS]
    state_at = done[0]
    long_at = done[1] + 1
    acts_at = long_at + LONG_TO_ACT
    last_slot = max(max(done), state_at + n_right, state_at + 5, acts_at) + 1

    def slot(t, carry):
        @pl.when((t > state_at) & (t <= state_at + n_right))
        def _():
            with jax.named_scope("ring"):
                state_ring(t - state_at)

        for g in range(3):
            s = t - OFFSETS[g]
            low = 1 if g == 0 else 0

            @pl.when((s >= low) & (s <= n_right + 2))
            def _():
                with jax.named_scope("comm%d" % g):
                    comm(g, s)

        @pl.when(t == 1)
        def _():
            border().wait_recv()
            for i in range(1, 8):
                border_share(i).start()

        @pl.when(t == 3)
        def _():
            wait_bytes(hr.at[1], 7 * 32 * 256 * 2)
            norm_rows(tok_edge, pl.ds(0, 32), pl.ds(t_rows, 32))

        for g in range(3):
            s = t - OFFSETS[g]

            @pl.when((s >= 2) & (s <= n_right + 2))
            def _():
                with jax.named_scope("share%d" % g):
                    share(g, s)

        @pl.when(t == state_at)
        def _():
            with jax.named_scope("lstate"):
                finish_a()
                local_state()
            for c in range(4):
                for way in (0, 1):
                    state_start(c, 1, way)

        @pl.when(t == done[1])
        def _():
            with jax.named_scope("fin_c"):
                finish_c()

        @pl.when(t == state_at + 1)
        def _():
            with jax.named_scope("read"):
                short_filter(384, 512, f_rd, c_ref)

        for i in range(4):
            @pl.when(t == state_at + 2 + i)
            def _():
                with jax.named_scope("inside"):
                    inside_strip(i)

        @pl.when(t == long_at)
        def _():
            with jax.named_scope("longf"):
                long_filter(0)

        @pl.when(t == long_at + 1)
        def _():
            with jax.named_scope("longf"):
                long_filter(1)
                send_sums()

        @pl.when(t == acts_at)
        def _():
            with jax.named_scope("fact"):
                filter_act()
        return carry

    lax.fori_loop(1, last_slot, slot, 0)
    border().wait_send()
    wait_bytes(hs.at[1], 7 * 32 * 256 * 2)

    entering = (e_left[...] * jnp.exp(run[0:1, :]) + e_right[...]).astype(BF16)
    for i in range(4):
        at = slice(128 * i, 128 * i + 128)
        carried = jnp.dot(c_ref[at, :], entering, preferred_element_type=F32)
        v = inside[at, :] + by_head(24, at) * carried
        g = gate_ref[at, :].astype(F32)
        v = v * (g * jax.nn.sigmoid(g))
        v = v * lax.rsqrt(jnp.mean(v * v, axis=-1, keepdims=True) + 1e-06)
        act[at, 0:256] = (v * out_gain[...]).astype(BF16)

    blocks = CHANNELS // 256

    def rows_of(xx, cc):
        return pl.ds(pl.multiple_of((2 * xx + cc) * 64, 64), 64)

    def at_x(k):
        return {"tp": 2 * lax.rem(x + k, 4) + core}

    def pair_copy(b):
        return remote(d2d_src.at[b], d2d_dst.at[b], os_.at[0], or_.at[0, b],
                      {"tp": 2 * x + 1 - core})

    def far_copy(b):
        return remote(far_src.at[b], far_dst.at[b], os_.at[1], or_.at[1, b],
                      at_x(1 + 2 * lax.rem(b, 2)))

    def relay_copy(b):
        return remote(rn_src.at[b], rn_dst.at[b], os_.at[2], or_.at[2, b],
                      at_x(1 + 2 * lax.rem(b, 2)))

    def direct_copy(b):
        return remote(dn_src.at[b], dn_dst.at[b], os_.at[3], or_.at[3, b],
                      at_x(3 + 2 * lax.rem(b, 2)))

    def stage_multiply(b):
        w = both(up, 2 * b, 2 * b + 1, 1)
        pbuf[b] = jnp.dot(act[...], w, preferred_element_type=F32)
        for xx in range(4):
            d2d_src[b, xx] = pbuf[b, rows_of(xx, 1 - core), :].astype(BF16)
        pair_copy(b).start()

    def stage_pair(b):
        pair_copy(b).wait_recv()
        for xx in range(4):
            at = rows_of(xx, core)
            pbuf[b, at, :] = pbuf[b, at, :] + d2d_dst[b, xx].astype(F32)
        far_src[b] = pbuf[b, rows_of(lax.rem(x + 2, 4), core), :].astype(BF16)
        far_copy(b).start()

    def stage_direct(b):
        dn_src[b] = pbuf[b, rows_of(lax.rem(x + 3 + 2 * lax.rem(b, 2), 4), core), :].astype(BF16)
        direct_copy(b).start()

    def stage_relay(b):
        far_copy(b).wait_recv()
        mine = pbuf[b, rows_of(lax.rem(x + 1 + 2 * lax.rem(b, 2), 4), core), :]
        rn_src[b] = (mine + far_dst[b].astype(F32)).astype(BF16)
        relay_copy(b).start()

    def stage_out(b):
        relay_copy(b).wait_recv()
        direct_copy(b).wait_recv()
        total = (pbuf[b, rows_of(x, core), :] + rn_dst[b].astype(F32)) + dn_dst[b].astype(F32)
        out[0, :, pl.ds(pl.multiple_of(b * 256, 256), 256)] = total.astype(BF16)

    def out_slot(i, carry):
        @pl.when(i < blocks)
        def _():
            with jax.named_scope("o_mm"):
                stage_multiply(i)

        for lag, stage in ((2, stage_pair), (5, stage_relay), (6, stage_direct), (9, stage_out)):
            @pl.when((i >= lag) & (i < blocks + lag))
            def _():
                with jax.named_scope("o_st%d" % lag):
                    stage(i - lag)
        return carry

    lax.fori_loop(0, blocks + 9, out_slot, 0)
    with jax.named_scope("o_end"):
        for k, r in enumerate((d2d_src, far_src, rn_src, dn_src)):
            pltpu.make_async_copy(r, r, os_.at[k]).wait()


def per_device(
    tokens, input_gain, weight_gate, weight_input, weight_write, weight_read, weight_step,
    weight_value, weight_sigmoid, filter_input, filter_write, filter_read, step_bias, rate_log,
    skip_gain, output_gain, opening_state, decay_shift, depth_filter, channel_gain,
    unproject_state, unproject_filter,
):
    n = lax.axis_size("sp")
    t = tokens.shape[1]
    hb = pl.BlockSpec(memory_space=pl.ANY)
    dma = pltpu.SemaphoreType.DMA
    steps = n // 2
    v = pltpu.VMEM
    return pl.pallas_call(
        partial(mixer_kernel, n),
        out_shape=jax.ShapeDtypeStruct((1, t // 8, CHANNELS), BF16),
        in_specs=[hb] * 22,
        out_specs=pl.BlockSpec(memory_space=pltpu.VMEM),
        scratch_shapes=[
            v((t, 2048), BF16), v((1, 2048), F32), v((4, 128), BF16),
            v((4, 256), BF16), v((4, 128), BF16), v((4, 128), BF16),
            *[pltpu.SMEM((4,), F32)] * 3,
            v((1, 256), F32), v((4, 64, 128), F32), v((4, t), F32), v((31, 256), BF16),
            v((1, 256), F32),
            v((n, t + 32, 128), BF16),
            v((n, 128, 512), BF16), v((n, 128, 256), BF16), v((n, 16, 128), BF16),
            v((n, 128, 384), BF16), v((n, 128, 128), BF16), v((n, 512, 128), BF16),
            v((t + 32, 768), F32), v((t + 32, 128), F32), v((t + 32, 512), F32),
            v((256, 256), BF16), v((31 * 8, 256), F32),
            v((32, 2048), BF16),
            v((8 + t, 512), F32), v((32 + t, 256), F32),
            v((t, 256), BF16), v((t, 128), BF16), v((t, 128), BF16), v((t, 256), BF16),
            v((128, t), F32), v((t, 128), F32), v((t, 256), F32), v((t, 256), F32),
            v((t, 128), F32),
            v((8, 8, t), F32), v((n, 128, 256), BF16), v((n, 8, 256), F32),
            v((128, 256), F32), v((128, 256), F32), v((8, 256), F32), v((t, 512), BF16),
            v((8, t, 256), F32), v((8, 4, 64, 256), BF16), v((8, 4, 64, 256), BF16),
            *[v((8, 64, 256), BF16)] * 6,
            dma((23,)), dma((3, 2, 4)), dma((7, 2, steps)),
            dma((3, 2, 4)), dma((3, 2, steps)),
            dma((2, 2)), dma((4, 2, steps)), dma((2,)), dma((2,)),
            dma((1,)), dma((1,)), dma((4,)), dma((4, 8)),
        ],
        compiler_params=pltpu.CompilerParams(
            collective_id=0, has_side_effects=True, vmem_limit_bytes=62 * 1024 * 1024),
        name="mixer",
    )(
        tokens, input_gain.reshape(1, -1), weight_input, weight_write, weight_step.T, weight_gate,
        weight_read, weight_value, weight_sigmoid, unproject_state, unproject_filter,
        filter_input, filter_write, filter_read, step_bias, rate_log, skip_gain,
        output_gain.reshape(1, -1), opening_state, decay_shift, depth_filter,
        channel_gain.reshape(1, -1),
    )


def solution(mesh):
    in_specs = (
        P("fs", "sp", None),
        P(),
        P("sp", "tp"),
        P("sp", "tp"),
        P("sp", "tp"),
        P("sp", "tp"),
        P("sp", "tp"),
        P("sp", "tp"),
        P("sp", "tp"),
        P(None, "tp"),
        P(None, "tp"),
        P(None, "tp"),
        P("tp"),
        P("tp"),
        P("tp"),
        P("tp"),
        P("fs", "tp", None, None),
        P("fs", "tp", "sp"),
        P(None, "tp"),
        P("tp"),
        P("tp", "sp"),
        P("tp", "sp"),
    )
    out_specs = P("fs", ("sp", "tp"), None)
    return jax.shard_map(
        per_device, mesh=mesh, in_specs=in_specs, out_specs=out_specs, check_vma=False
    )
```

```python
from functools import partial

import jax
import jax.numpy as jnp
from jax import lax
from jax.experimental import pallas as pl
from jax.experimental.pallas import tpu as pltpu
from jax.sharding import PartitionSpec as P

MESH = pl.DeviceIdType.MESH
F32, BF16 = jnp.float32, jnp.bfloat16
CHANNELS = 2048
OFFSETS = (0, 2, 6)
SHARE_LAGS = (1, 2, 2)


def mixer_kernel(
    n,
    tok_h, gain_h, wi, ww, ws_h, wg, wr, wv, wsg, us, uf,
    f_in_h, f_wr_h, f_rd_h, bias_h, rate_h, skip_h, out_gain_h, opening_h, shift_h, taps_h,
    ch_gain_h,
    out,
    tok, gain, ws_v, f_in, f_wr, f_rd, bias, rate, skip, out_gain, opening, shift, taps, ch_gain,
    normed, ap, aq, as_, cp, cq, up, gp, acc_a, acc_q, acc_s, acc_c, acc_g, blank, tapsb,
    tok_edge, ext4, extq, ext31, x_ref, b_ref, c_ref,
    rows_ref, cols_ref, inside, filtered, sums_ref, stat, ebuf, tbuf, e_right, e_left, run, act,
    pbuf, d2d_src, d2d_dst, far_src, far_dst, rn_src, rn_dst, dn_src, dn_dst,
    local_sem, zs, zr, ys, yr, yds, ydr, es, er, hs, hr, ss, sr, os_, or_,
):
    z = lax.axis_index("sp")
    y = lax.axis_index("fs")
    tp = lax.axis_index("tp")
    x, core = tp // 2, lax.rem(tp, 2)
    n_right, n_left = n // 2, (n - 1) // 2
    z_next, z_prev = lax.rem(z + 1, n), lax.rem(z + n - 1, n)
    y_next, y_prev = lax.rem(y + 1, 4), lax.rem(y + 3, 4)
    t_rows = tok.shape[0]

    barrier = pltpu.get_barrier_semaphore()
    greet = [{"sp": z_next}, {"sp": z_prev}, {"fs": y_next}, {"fs": y_prev}]
    greet += [{"tp": lax.rem(tp + i, 8)} for i in range(1, 8)]
    for where in greet:
        pl.semaphore_signal(barrier, inc=1, device_id=where, device_id_type=MESH)

    pairs = [
        (ws_h, ws_v), (wi, ap.at[z]),
        (ww, aq.at[z, :, pl.ds(0, 128)]), (wr, aq.at[z, :, pl.ds(128, 128)]),
        (tok_h.at[0], tok), (gain_h, gain), (wg, gp.at[z]), (wv, cp.at[z, :, pl.ds(0, 256)]),
        (wsg.at[:, pl.ds(0, 128)], cp.at[z, :, pl.ds(256, 128)]),
        (wsg.at[:, pl.ds(128, 128)], cq.at[z]),
        (us, up.at[z, pl.ds(0, 256)]), (uf, up.at[z, pl.ds(256, 256)]),
        (f_in_h, f_in), (f_wr_h, f_wr), (f_rd_h, f_rd), (bias_h, bias), (rate_h, rate),
        (skip_h, skip), (out_gain_h, out_gain), (opening_h.at[0], opening),
        (shift_h.at[0], shift), (taps_h, taps), (ch_gain_h, ch_gain),
    ]
    own = [pltpu.make_async_copy(s, d, local_sem.at[k]) for k, (s, d) in enumerate(pairs)]
    for c in own:
        c.start()

    def remote(src, dst, send, recv, where):
        return pltpu.make_async_remote_copy(
            src_ref=src, dst_ref=dst, send_sem=send, recv_sem=recv, device_id=where,
            device_id_type=MESH)

    def wait_bytes(sem, count):
        ref = blank.at[pl.ds(0, count // 512)]
        pltpu.make_async_copy(ref, ref, sem).wait()

    groups = [((ap,), (aq, as_)), ((cp,), (cq,)), ((up, gp), ())]
    q_parts = (4, 2, 0)
    part_bytes = [sum(ref.shape[1] // 4 * ref.shape[2] * 2 for ref in two) for two, _ in groups]
    z_bytes = [p + sum(ref.shape[1] * ref.shape[2] * 2 for ref in one)
               for p, (_, one) in zip(part_bytes, groups)]

    def shard(s, way):
        return lax.rem(z + n - s, n) if way == 0 else lax.rem(z + s, n)

    def part(buf, j, q):
        rows = buf.shape[1] // 4
        return buf.at[j, pl.ds(pl.multiple_of(q * rows, rows), rows)]

    def pieces(g, c, j):
        two, one = groups[g]
        if c < len(two):
            return [part(two[len(two) - 1 - c], j, y)]
        rows = one[0].shape[1] // q_parts[g]
        more = [b.at[j] for b in one[1:]] if c == chunks[g] - 1 else []
        return [one[0].at[j, pl.ds((c - len(two)) * rows, rows)]] + more

    chunks = [len(two) + q for (two, _), q in zip(groups, q_parts)]
    first = [sum(chunks[:g]) for g in range(len(groups))]

    def chunk_bytes(g, c):
        two, one = groups[g]
        if c < len(two):
            ref = two[len(two) - 1 - c]
            return ref.shape[1] // 4 * ref.shape[2] * 2
        rest = sum(r.shape[1] * r.shape[2] * 2 for r in one[1:]) if c == chunks[g] - 1 else 0
        return one[0].shape[1] * one[0].shape[2] * 2 // q_parts[g] + rest

    def start_chunk(g, c, s, way):
        for r in pieces(g, c, shard(s - 1, way)):
            remote(r, r, zs.at[g, way, lax.rem(s, 4)], zr.at[first[g] + c, way, lax.rem(s, 4)],
                   {"sp": z_next if way == 0 else z_prev}).start()

    y_far = lax.rem(y + 2, 4)
    direct_from = n_right
    finals = (n_right + 1, n_right + 3, n_right + 3)

    def y_start(g, s, way, kind, q):
        up_way = kind == 0 or (kind == 2 and way == 0)
        k = kind // 2
        where = y_far if kind == 3 else (y_next if up_way else y_prev)
        for ref in groups[g][0]:
            r = part(ref, shard(s, way), q)
            if kind == 3:
                remote(r, r, yds.at[g], ydr.at[g], {"fs": where}).start()
            else:
                remote(r, r, ys.at[g, k, lax.rem(s, 4)], yr.at[g, k, s - 1],
                       {"fs": where}).start()

    def y_wait(sem, g, s, per_way):
        @pl.when(s <= n_left)
        def _():
            wait_bytes(sem, 2 * per_way * part_bytes[g])

        @pl.when(s > n_left)
        def _():
            wait_bytes(sem, per_way * part_bytes[g])

    def comm(g, s):
        for c in range(chunks[g]):
            for way in (0, 1):
                last = (n_right, n_left)[way]

                @pl.when((s >= 1) & (s <= last))
                def _():
                    wait_bytes(zr.at[first[g] + c, way, lax.rem(s, 4)], chunk_bytes(g, c))

                @pl.when(s < last)
                def _():
                    start_chunk(g, c, s + 1, way)

                if c == len(groups[g][0]) - 1:
                    @pl.when((s >= 1) & (s <= last))
                    def _():
                        y_start(g, s, way, 0, y)
                        y_start(g, s, way, 1, y)

                        @pl.when(s >= direct_from)
                        def _():
                            y_start(g, s, way, 3, y)

        @pl.when((s >= 3) & (s <= n_right + 2))
        def _():
            wait_bytes(zs.at[g, 0, lax.rem(s - 2, 4)], z_bytes[g])

            @pl.when(s - 2 <= n_left)
            def _():
                wait_bytes(zs.at[g, 1, lax.rem(s - 2, 4)], z_bytes[g])

    def share(g, s):
        lag = SHARE_LAGS[g]
        final = finals[g]

        @pl.when((s >= 1 + lag) & (s <= n_right + lag))
        def _():
            y_wait(yr.at[g, 0, s - lag - 1], g, s - lag, 2)
            y_wait(ys.at[g, 0, lax.rem(s - lag, 4)], g, s - lag, 2)

            @pl.when(s - lag < direct_from)
            def _():
                y_start(g, s - lag, 0, 2, y_prev)
                y_start(g, s - lag, 1, 2, y_next)

        @pl.when((s >= 2 + lag) & (s <= direct_from + lag))
        def _():
            wait_bytes(ys.at[g, 1, lax.rem(s - lag - 1, 4)], 2 * part_bytes[g])

        def complete(k, carry):
            @pl.when(k < direct_from)
            def _():
                wait_bytes(yr.at[g, 1, k - 1], 2 * part_bytes[g])

            @pl.when(k == direct_from)
            def _():
                wait_bytes(ydr.at[g], part_bytes[g])
                wait_bytes(yds.at[g], part_bytes[g])

            with jax.named_scope("mm"):
                multiply(g, k)
            return carry

        @pl.when((s >= 3 + lag) & (s <= final))
        def _():
            low, high = s - 2 - lag, jnp.where(s == final, n_right, s - 2 - lag)
            if g == 0:
                low = jnp.where(s == final, low + 1, low)
                high = jnp.where(s == final - 1, high + 1, high)
            lax.fori_loop(low, high + 1, complete, 0)

    def both(ref, j1, j2, axis):
        return jnp.concatenate([ref[j1], ref[j2]], axis=axis)

    def rows_at(k):
        j1 = jnp.where(k == n_right, z, shard(k, 0))
        j2 = shard(k, 1)
        return j1, j2, both(normed, j1, j2, 1)

    def multiply_early(k):
        j1, j2, rows = rows_at(k)
        acc_q[...] += jnp.dot(rows, both(aq, j1, j2, 0), preferred_element_type=F32)
        acc_s[:, :16] += lax.dot_general(
            rows, both(as_, j1, j2, 1), (((1,), (1,)), ((), ())), preferred_element_type=F32)

    def multiply(g, k):
        j1, j2, rows = rows_at(k)
        if g == 0:
            acc_a[...] += jnp.dot(rows, both(ap, j1, j2, 0), preferred_element_type=F32)
        elif g == 2:
            acc_g[...] += jnp.dot(rows[:t_rows], both(gp, j1, j2, 0), preferred_element_type=F32)
        else:
            w = jnp.concatenate([both(cp, j1, j2, 0), both(cq, j1, j2, 0)], axis=1)
            acc_c[...] += jnp.dot(rows, w, preferred_element_type=F32)

    edge_lanes = pl.ds(pl.multiple_of(tp * 256, 256), 256)

    def border():
        return remote(tok.at[pl.ds(t_rows - 32, 32), edge_lanes], tok_edge.at[:, edge_lanes],
                      hs.at[0], hr.at[0], {"sp": z_next})

    def border_share(i):
        ref = tok_edge.at[:, edge_lanes]
        return remote(ref, ref, hs.at[1], hr.at[1], {"tp": lax.rem(tp + i, 8)})

    def short_filter(source, lo, hi, kernel, target):
        weights = [kernel[k:k + 1, :].astype(F32) for k in range(4)]

        def strip(i, carry):
            block = source[pl.ds(pl.multiple_of(i * 64, 64), 72), lo:hi]
            total = weights[0] * pltpu.roll(block, 72 - 5, 0)[:64]
            for k in range(1, 4):
                total = total + weights[k] * pltpu.roll(block, 72 - 5 - k, 0)[:64]
            target[pl.ds(pl.multiple_of(i * 64, 64), 64), :] = (
                total * jax.nn.sigmoid(total)).astype(BF16)
            return carry

        lax.fori_loop(0, t_rows // 64, strip, 0)

    def extend(target, acc, lo, hi):
        target[0:8, :] = jnp.where(z > 0, acc[t_rows + 24:, lo:hi].astype(BF16).astype(F32), 0.0)
        target[8:, :] = acc[0:t_rows, lo:hi].astype(BF16).astype(F32)

    def finish_c():
        value = acc_c[:, :256].astype(BF16).astype(F32)
        sig = acc_c[:, 256:].astype(BF16).astype(F32)
        glu = (value * jax.nn.sigmoid(sig)).astype(BF16).astype(F32)
        ext31[0:32, :] = jnp.where(z > 0, glu[t_rows:], 0.0)
        ext31[32:, :] = glu[:t_rows]

    lane = lax.broadcasted_iota(jnp.int32, (1, 128), 1)

    def by_head(first, rows=slice(None)):
        c = cols_ref[rows, first:first + 4]
        return jnp.concatenate(
            [jnp.where(lane < 64, c[:, 2 * k:2 * k + 1], c[:, 2 * k + 1:2 * k + 2])
             for k in range(2)], axis=1)

    def local_rates():
        extend(extq, acc_q, 0, 256)
        short_filter(extq, 0, 128, f_wr, b_ref)
        short_filter(extq, 128, 256, f_rd, c_ref)
        head = lax.broadcasted_iota(jnp.int32, (8, t_rows), 0)
        place = lax.broadcasted_iota(jnp.int32, (8, t_rows), 1)
        bias8 = jnp.zeros((8, t_rows), F32)
        rate8 = jnp.zeros((8, t_rows), F32)
        for h in range(4):
            bias8 = jnp.where(head == h, bias[h], bias8)
            rate8 = jnp.where(head == h, rate[h], rate8)
        steps = acc_s[0:t_rows, :].astype(BF16).astype(F32).T[:8] + bias8
        steps = jnp.maximum(steps, 0.0) + jnp.log1p(jnp.exp(-jnp.abs(steps)))
        rows_ref[0:4, :] = shift[...]
        rows_ref[4:8, :] = jnp.zeros((4, t_rows), F32)
        total = rows_ref[0:8, :] - steps * jnp.exp(rate8)
        k = 1
        while k < t_rows:
            total = total + jnp.where(place >= k, pltpu.roll(total, k, 1), 0.0)
            k *= 2
        end = total[:, t_rows - 1:t_rows]
        rows_ref[0:8, :] = total
        rows_ref[8:16, :] = steps
        rows_ref[16:24, :] = steps * jnp.exp(end - total)
        rows_ref[24:32, :] = jnp.exp(total)
        rows_ref[32:, :] = jnp.zeros((96, t_rows), F32)
        cols_ref[...] = rows_ref[...].T
        spread = jnp.concatenate(
            [jnp.where(lane < 64, end[2 * k:2 * k + 1, :], end[2 * k + 1:2 * k + 2, :])
             for k in range(2)], axis=1)
        tbuf[z] = jnp.broadcast_to(spread, (8, 256))

    def local_state():
        extend(ext4, acc_a, 0, 256)
        short_filter(ext4, 0, 256, f_in, x_ref)
        scaled = (x_ref[...].astype(F32) * by_head(16)).astype(BF16)
        ebuf[z] = lax.dot_general(
            b_ref[...], scaled, (((0,), (0,)), ((), ())), preferred_element_type=F32
        ).astype(BF16)

    e_bytes = (2 * 32 * 256 + 4 * 8 * 256,) + (2 * 32 * 256,) * 3

    def state_start(c, s, way):
        j = shard(s - 1, way)
        where = {"sp": z_next if way == 0 else z_prev}
        for r in [ebuf.at[j, pl.ds(32 * c, 32)]] + [tbuf.at[j]] * (c == 0):
            remote(r, r, es.at[way, lax.rem(s, 2)], er.at[c, way, lax.rem(s, 4)], where).start()

    def state_ring(s):
        for c in range(4):
            for way in (0, 1):
                last = (n_right, n_left)[way]

                @pl.when(s <= last)
                def _():
                    wait_bytes(er.at[c, way, lax.rem(s, 4)], e_bytes[c])

                @pl.when(s < last)
                def _():
                    state_start(c, s + 1, way)

        for way in (0, 1):
            last = (n_right, n_left)[way]

            @pl.when(s <= last)
            def _():
                j = shard(s, way)
                total = tbuf[j][0:1]
                if way == 0:
                    @pl.when(z >= s)
                    def _():
                        e_right[...] += jnp.exp(run[0:1, :]) * ebuf[j].astype(F32)
                        run[...] += total
                else:
                    @pl.when(z + s >= n)
                    def _():
                        e_left[...] = e_left[...] * jnp.exp(total) + ebuf[j].astype(F32)
                wait_bytes(es.at[way, lax.rem(s, 2)], sum(e_bytes))

    def inside_strip(i):
        k = 128 * (i + 1)
        at = slice(128 * i, k)
        scores = lax.dot_general(
            c_ref[at, :], b_ref[0:k, :], (((1,), (1,)), ((), ())), preferred_element_type=F32)
        diag = (lax.broadcasted_iota(jnp.int32, (128, k), 0) + 128 * i
                >= lax.broadcasted_iota(jnp.int32, (128, k), 1))
        pieces = []
        for h in range(4):
            gap = cols_ref[at, h:h + 1] - rows_ref[h:h + 1, 0:k]
            decay = jnp.exp(jnp.where(diag, gap, -jnp.inf)) * rows_ref[8 + h:9 + h, 0:k]
            tile = slice(128 * (h // 2), 128 * (h // 2) + 128)
            pieces.append(jnp.dot((scores * decay).astype(BF16), x_ref[0:k, tile],
                                  preferred_element_type=F32))
        for k in range(2):
            gains = jnp.where(lane < 64, skip[2 * k], skip[2 * k + 1])
            lanes = slice(128 * k, 128 * k + 128)
            inside[at, lanes] = (jnp.where(lane < 64, pieces[2 * k], pieces[2 * k + 1])
                                 + gains * x_ref[at, lanes].astype(F32))

    def stat_copy(i):
        return remote(stat.at[tp], stat.at[tp], ss.at[0], sr.at[0], {"tp": lax.rem(tp + i, 8)})

    def long_filter(half):
        def strip(i, carry):
            block = ext31[pl.ds(pl.multiple_of(i * 64, 64), 96), :]
            total = jnp.zeros((8, 8, 256), F32)
            for r in range(8):
                moved = block if r == 0 else pltpu.roll(block, 96 - r, 0)
                for a in range(5):
                    k = 8 * a + r - 2
                    if 0 <= k < 31:
                        total = total + (tapsb[8 * k:8 * k + 8, :][None]
                                         * moved[8 * a:8 * a + 64].reshape(8, 8, 256))
            total = total.reshape(64, 256)
            at = pl.ds(pl.multiple_of(i * 64, 64), 64)
            filtered[at, :] = total
            sum1 = jnp.sum(total, axis=1, keepdims=True)
            sum2 = jnp.sum(total * total, axis=1, keepdims=True)
            sums_ref[at, :] = jnp.where(lane == 0, sum1, jnp.where(lane == 1, sum2, 0.0))
            return carry

        lax.fori_loop(half * (t_rows // 128), (half + 1) * (t_rows // 128), strip, 0)

    def send_sums():
        stat[tp] = sums_ref[...].T[0:8]
        for i in range(1, 8):
            stat_copy(i).start()

    def filter_act():
        with jax.named_scope("fact_wait"):
            wait_bytes(sr.at[0], 7 * 8 * t_rows * 4)
        sums = stat[0]
        for i in range(1, 8):
            sums = sums + stat[i]
        mean = sums[0:1] / CHANNELS
        var = sums[1:2] / CHANNELS - mean * mean
        rows_ref[32:33, :] = mean
        rows_ref[33:34, :] = lax.rsqrt(var + 1e-05)
        sums_ref[...] = rows_ref[...].T

        def strip(i, carry):
            at = pl.ds(pl.multiple_of(i * 64, 64), 64)
            f = (filtered[at, :] - sums_ref[at, 32:33]) * sums_ref[at, 33:34] * ch_gain[...]
            act[at, 256:512] = (f * jax.nn.sigmoid(f)).astype(BF16)
            return carry

        lax.fori_loop(0, t_rows // 64, strip, 0)
        wait_bytes(ss.at[0], 7 * 8 * t_rows * 4)

    own[0].wait()
    as_[z] = jnp.concatenate([ws_v[...].astype(F32), jnp.zeros((12, 128), F32)]).astype(BF16)
    for c in own[1:4]:
        c.wait()
    with jax.named_scope("entry"):
        pl.semaphore_wait(barrier, len(greet))
    for c in range(chunks[0]):
        start_chunk(0, c, 1, 0)
        start_chunk(0, c, 1, 1)
    for c in own[4:]:
        c.wait()

    border().start()

    def norm_rows(source, at, to):
        v = source[at, :].astype(F32)
        scale = lax.rsqrt(jnp.mean(v * v, axis=-1, keepdims=True) + 1e-06)
        v = (v * scale * gain[...]).astype(BF16)
        for j in range(n):
            normed[j, to, :] = v[:, j * 128:(j + 1) * 128]

    def norm_strip(i, carry):
        at = pl.ds(pl.multiple_of(i * 32, 32), 32)
        norm_rows(tok, at, at)
        return carry

    with jax.named_scope("norm"):
        lax.fori_loop(0, t_rows // 32, norm_strip, 0)
    e_right[...] = jnp.zeros_like(e_right)
    run[...] = jnp.zeros_like(run)
    e_left[...] = opening[...].reshape(256, 128).T
    for acc in (acc_a, acc_q, acc_s, acc_c, acc_g):
        acc[...] = jnp.zeros_like(acc)
    for k in range(taps.shape[0]):
        tapsb[8 * k:8 * k + 8, :] = jnp.broadcast_to(
            taps[k:k + 1, :].astype(F32), (8, 256))

    done = [f + o for f, o in zip(finals, OFFSETS)]
    state_at = done[0]
    long_at = done[1] + 1
    last_slot = max(max(done), state_at + n_right, state_at + 5, long_at + 2) + 1

    assert long_at + 1 < state_at + n_right and last_slot == state_at + n_right + 1

    def at_step(g, t):
        return t - OFFSETS[g] - (jnp.where(t > state_at, 0, 1) if g == 2 else 0)

    def slot(t, carry):
        @pl.when(t == state_at + n_right)
        def _():
            with jax.named_scope("fact"):
                filter_act()

        @pl.when((t > state_at) & (t <= state_at + n_right))
        def _():
            with jax.named_scope("ring"):
                state_ring(t - state_at)

        for g in range(3):
            s = at_step(g, t)
            low = 1 if g == 0 else 0

            @pl.when((s >= low) & (s <= n_right + 2))
            def _():
                with jax.named_scope("comm%d" % g):
                    comm(g, s)

        @pl.when(t == 1)
        def _():
            border().wait_recv()
            for i in range(1, 8):
                border_share(i).start()

        @pl.when(t == 3)
        def _():
            wait_bytes(hr.at[1], 7 * 32 * 256 * 2)
            norm_rows(tok_edge, pl.ds(0, 32), pl.ds(t_rows, 32))

        def early(k, carry):
            multiply_early(k)
            return carry

        @pl.when((t >= 3) & (t <= n_right))
        def _():
            with jax.named_scope("mmq"):
                lax.fori_loop(jnp.where(t == 3, 1, t), t + 1, early, 0)

        @pl.when(t == n_right + 1)
        def _():
            with jax.named_scope("rates"):
                local_rates()

        for i in range(4):
            @pl.when(t == state_at + 1 + i)
            def _():
                with jax.named_scope("inside"):
                    inside_strip(i)

        for i in range(2):
            @pl.when(t == long_at + i)
            def _():
                with jax.named_scope("longf"):
                    long_filter(i)
                    if i == 1:
                        send_sums()

        for g in range(3):
            s = at_step(g, t)

            @pl.when((s >= 2) & (s <= finals[g]))
            def _():
                with jax.named_scope("share%d" % g):
                    share(g, s)

        @pl.when(t == state_at)
        def _():
            with jax.named_scope("lstate"):
                local_state()
            for c in range(4):
                for way in (0, 1):
                    state_start(c, 1, way)
            with jax.named_scope("extra"):
                comm(2, state_at - OFFSETS[2])
                share(2, state_at - OFFSETS[2])

        @pl.when(t == done[1])
        def _():
            with jax.named_scope("fin_c"):
                finish_c()
        return carry

    lax.fori_loop(1, last_slot, slot, 0)
    border().wait_send()
    wait_bytes(hs.at[1], 7 * 32 * 256 * 2)

    entering = (e_left[...] * jnp.exp(run[0:1, :]) + e_right[...]).astype(BF16)
    for i in range(4):
        at = slice(128 * i, 128 * i + 128)
        carried = jnp.dot(c_ref[at, :], entering, preferred_element_type=F32)
        v = inside[at, :] + by_head(24, at) * carried
        g = acc_g[at, :].astype(BF16).astype(F32)
        v = v * (g * jax.nn.sigmoid(g))
        v = v * lax.rsqrt(jnp.mean(v * v, axis=-1, keepdims=True) + 1e-06)
        act[at, 0:256] = (v * out_gain[...]).astype(BF16)

    blocks = CHANNELS // 256

    def rows_of(xx, cc):
        return pl.ds(pl.multiple_of((2 * xx + cc) * 64, 64), 64)

    def at_x(k):
        return {"tp": 2 * lax.rem(x + k, 4) + core}

    def pair_copy(b):
        return remote(d2d_src.at[b], d2d_dst.at[b], os_.at[0], or_.at[0, b],
                      {"tp": 2 * x + 1 - core})

    def far_copy(b):
        return remote(far_src.at[b], far_dst.at[b], os_.at[1], or_.at[1, b],
                      at_x(1 + 2 * lax.rem(b, 2)))

    def relay_copy(b):
        return remote(rn_src.at[b], rn_dst.at[b], os_.at[2], or_.at[2, b],
                      at_x(1 + 2 * lax.rem(b, 2)))

    def direct_copy(b):
        return remote(dn_src.at[b], dn_dst.at[b], os_.at[3], or_.at[3, b],
                      at_x(3 + 2 * lax.rem(b, 2)))

    def stage_multiply(b):
        w = both(up, 2 * b, 2 * b + 1, 1)
        pbuf[b] = jnp.dot(act[...], w, preferred_element_type=F32)
        for xx in range(4):
            d2d_src[b, xx] = pbuf[b, rows_of(xx, 1 - core), :].astype(BF16)
        pair_copy(b).start()

    def stage_pair(b):
        pair_copy(b).wait_recv()
        for xx in range(4):
            at = rows_of(xx, core)
            pbuf[b, at, :] = pbuf[b, at, :] + d2d_dst[b, xx].astype(F32)
        far_src[b] = pbuf[b, rows_of(lax.rem(x + 2, 4), core), :].astype(BF16)
        far_copy(b).start()

    def stage_direct(b):
        dn_src[b] = pbuf[b, rows_of(lax.rem(x + 3 + 2 * lax.rem(b, 2), 4), core), :].astype(BF16)
        direct_copy(b).start()

    def stage_relay(b):
        far_copy(b).wait_recv()
        mine = pbuf[b, rows_of(lax.rem(x + 1 + 2 * lax.rem(b, 2), 4), core), :]
        rn_src[b] = (mine + far_dst[b].astype(F32)).astype(BF16)
        relay_copy(b).start()

    def stage_out(b):
        relay_copy(b).wait_recv()
        direct_copy(b).wait_recv()
        total = (pbuf[b, rows_of(x, core), :] + rn_dst[b].astype(F32)) + dn_dst[b].astype(F32)
        out[0, :, pl.ds(pl.multiple_of(b * 256, 256), 256)] = total.astype(BF16)

    def out_slot(i, carry):
        @pl.when(i < blocks)
        def _():
            with jax.named_scope("o_mm"):
                stage_multiply(i)

        for lag, stage in ((3, stage_pair), (9, stage_direct), (10, stage_relay), (18, stage_out)):
            @pl.when((i >= lag) & (i < blocks + lag))
            def _():
                with jax.named_scope("o_st%d" % lag):
                    stage(i - lag)
        return carry

    lax.fori_loop(0, blocks + 18, out_slot, 0)
    with jax.named_scope("o_end"):
        for k, r in enumerate((d2d_src, far_src, rn_src, dn_src)):
            pltpu.make_async_copy(r, r, os_.at[k]).wait()


def per_device(
    tokens, input_gain, weight_gate, weight_input, weight_write, weight_read, weight_step,
    weight_value, weight_sigmoid, filter_input, filter_write, filter_read, step_bias, rate_log,
    skip_gain, output_gain, opening_state, decay_shift, depth_filter, channel_gain,
    unproject_state, unproject_filter,
):
    n = lax.axis_size("sp")
    t = tokens.shape[1]
    hb = pl.BlockSpec(memory_space=pl.ANY)
    dma = pltpu.SemaphoreType.DMA
    steps = n // 2
    v = pltpu.VMEM
    return pl.pallas_call(
        partial(mixer_kernel, n),
        out_shape=jax.ShapeDtypeStruct((1, t // 8, CHANNELS), BF16),
        in_specs=[hb] * 22,
        out_specs=pl.BlockSpec(memory_space=pltpu.VMEM),
        scratch_shapes=[
            v((t, 2048), BF16), v((1, 2048), F32), v((4, 128), BF16),
            v((4, 256), BF16), v((4, 128), BF16), v((4, 128), BF16),
            *[pltpu.SMEM((4,), F32)] * 3,
            v((1, 256), F32), v((4, 64, 128), F32), v((4, t), F32), v((31, 256), BF16),
            v((1, 256), F32),
            v((n, t + 32, 128), BF16),
            v((n, 128, 256), BF16), v((n, 128, 256), BF16), v((n, 16, 128), BF16),
            v((n, 128, 384), BF16), v((n, 128, 128), BF16), v((n, 512, 128), BF16),
            v((n, 128, 256), BF16),
            v((t + 32, 256), F32), v((t + 32, 256), F32), v((t + 32, 128), F32), v((t + 32, 512), F32),
            v((t, 256), F32),
            v((384, 256), BF16), v((31 * 8, 256), F32),
            v((32, 2048), BF16),
            v((8 + t, 256), F32), v((8 + t, 256), F32), v((32 + t, 256), F32),
            v((t, 256), BF16), v((t, 128), BF16), v((t, 128), BF16),
            v((128, t), F32), v((t, 128), F32), v((t, 256), F32), v((t, 256), F32),
            v((t, 128), F32),
            v((8, 8, t), F32), v((n, 128, 256), BF16), v((n, 8, 256), F32),
            v((128, 256), F32), v((128, 256), F32), v((8, 256), F32), v((t, 512), BF16),
            v((8, t, 256), F32), v((8, 4, 64, 256), BF16), v((8, 4, 64, 256), BF16),
            *[v((8, 64, 256), BF16)] * 6,
            dma((23,)), dma((3, 2, 4)), dma((10, 2, 4)),
            dma((3, 2, 4)), dma((3, 2, steps)), dma((3,)), dma((3,)),
            dma((2, 2)), dma((4, 2, 4)), dma((2,)), dma((2,)),
            dma((1,)), dma((1,)), dma((4,)), dma((4, 8)),
        ],
        compiler_params=pltpu.CompilerParams(
            collective_id=0, has_side_effects=True, vmem_limit_bytes=62 * 1024 * 1024),
        name="mixer",
    )(
        tokens, input_gain.reshape(1, -1), weight_input, weight_write, weight_step.T, weight_gate,
        weight_read, weight_value, weight_sigmoid, unproject_state, unproject_filter,
        filter_input, filter_write, filter_read, step_bias, rate_log, skip_gain,
        output_gain.reshape(1, -1), opening_state, decay_shift, depth_filter,
        channel_gain.reshape(1, -1),
    )


def solution(mesh):
    in_specs = (
        P("fs", "sp", None),
        P(),
        P("sp", "tp"),
        P("sp", "tp"),
        P("sp", "tp"),
        P("sp", "tp"),
        P("sp", "tp"),
        P("sp", "tp"),
        P("sp", "tp"),
        P(None, "tp"),
        P(None, "tp"),
        P(None, "tp"),
        P("tp"),
        P("tp"),
        P("tp"),
        P("tp"),
        P("fs", "tp", None, None),
        P("fs", "tp", "sp"),
        P(None, "tp"),
        P("tp"),
        P("tp", "sp"),
        P("tp", "sp"),
    )
    out_specs = P("fs", ("sp", "tp"), None)
    return jax.shard_map(
        per_device, mesh=mesh, in_specs=in_specs, out_specs=out_specs, check_vma=False
    )
```

```python
from functools import partial

import jax
import jax.numpy as jnp
from jax import lax
from jax.experimental import pallas as pl
from jax.experimental.pallas import tpu as pltpu
from jax.sharding import PartitionSpec as P

MESH = pl.DeviceIdType.MESH
F32, BF16 = jnp.float32, jnp.bfloat16
CHANNELS = 2048
OFFSETS = (0, 2, 6)
SHARE_LAGS = (1, 2, 2)


def mixer_kernel(
    n,
    tok_h, gain_h, wi, ww, ws_h, wg, wr, wv, wsg, us, uf,
    f_in_h, f_wr_h, f_rd_h, bias_h, rate_h, skip_h, out_gain_h, opening_h, shift_h, taps_h,
    ch_gain_h,
    out,
    tok, gain, ws_v, f_in, f_wr, f_rd, bias, rate, skip, out_gain, opening, shift, taps, ch_gain,
    normed, ap, aq, as_, cp, cq, up, uq, gp, acc_a, acc_q, acc_s, acc_c, acc_g, blank, tapsb,
    tok_edge, ext4, extq, ext31, x_ref, b_ref, c_ref,
    rows_ref, cols_ref, inside, filtered, sums_ref, stat, ebuf, tbuf, e_right, e_left, run, act,
    pbuf, d2d_src, d2d_dst, far_src, far_dst, rn_src, rn_dst, dn_src, dn_dst,
    local_sem, zs, zr, ys, yr, yds, ydr, es, er, hs, hr, ss, sr, os_, or_,
):
    z = lax.axis_index("sp")
    y = lax.axis_index("fs")
    tp = lax.axis_index("tp")
    x, core = tp // 2, lax.rem(tp, 2)
    n_right, n_left = n // 2, (n - 1) // 2
    z_next, z_prev = lax.rem(z + 1, n), lax.rem(z + n - 1, n)
    y_next, y_prev = lax.rem(y + 1, 4), lax.rem(y + 3, 4)
    t_rows = tok.shape[0]

    barrier = pltpu.get_barrier_semaphore()
    greet = [{"sp": z_next}, {"sp": z_prev}, {"fs": y_next}, {"fs": y_prev}]
    greet += [{"tp": lax.rem(tp + i, 8)} for i in range(1, 8)]
    for where in greet:
        pl.semaphore_signal(barrier, inc=1, device_id=where, device_id_type=MESH)

    pairs = [
        (ws_h, ws_v), (wi, ap.at[z]),
        (ww, aq.at[z, :, pl.ds(0, 128)]), (wr, aq.at[z, :, pl.ds(128, 128)]),
        (tok_h.at[0], tok), (gain_h, gain), (wg, gp.at[z]), (wv, cp.at[z, :, pl.ds(0, 256)]),
        (wsg.at[:, pl.ds(0, 128)], cp.at[z, :, pl.ds(256, 128)]),
        (wsg.at[:, pl.ds(128, 128)], cq.at[z]),
        (us, up.at[z, pl.ds(0, 256)]), (uf.at[pl.ds(0, 192)], up.at[z, pl.ds(256, 192)]),
        (uf.at[pl.ds(192, 64)], uq.at[z]),
        (f_in_h, f_in), (f_wr_h, f_wr), (f_rd_h, f_rd), (bias_h, bias), (rate_h, rate),
        (skip_h, skip), (out_gain_h, out_gain), (opening_h.at[0], opening),
        (shift_h.at[0], shift), (taps_h, taps), (ch_gain_h, ch_gain),
    ]
    own = [pltpu.make_async_copy(s, d, local_sem.at[k]) for k, (s, d) in enumerate(pairs)]
    for c in own:
        c.start()

    def remote(src, dst, send, recv, where):
        return pltpu.make_async_remote_copy(
            src_ref=src, dst_ref=dst, send_sem=send, recv_sem=recv, device_id=where,
            device_id_type=MESH)

    def wait_bytes(sem, count):
        ref = blank.at[pl.ds(0, count // 512)]
        pltpu.make_async_copy(ref, ref, sem).wait()

    groups = [((ap,), (aq, as_)), ((cp,), (cq,)), ((up, gp), (uq,))]
    q_parts = (4, 2, 1)
    part_bytes = [sum(ref.shape[1] // 4 * ref.shape[2] * 2 for ref in two) for two, _ in groups]
    z_bytes = [p + sum(ref.shape[1] * ref.shape[2] * 2 for ref in one)
               for p, (_, one) in zip(part_bytes, groups)]

    def shard(s, way):
        return lax.rem(z + n - s, n) if way == 0 else lax.rem(z + s, n)

    def part(buf, j, q):
        rows = buf.shape[1] // 4
        return buf.at[j, pl.ds(pl.multiple_of(q * rows, rows), rows)]

    def pieces(g, c, j):
        two, one = groups[g]
        if c < len(two):
            return [part(two[len(two) - 1 - c], j, y)]
        rows = one[0].shape[1] // q_parts[g]
        more = [b.at[j] for b in one[1:]] if c == chunks[g] - 1 else []
        return [one[0].at[j, pl.ds((c - len(two)) * rows, rows)]] + more

    chunks = [len(two) + q for (two, _), q in zip(groups, q_parts)]
    first = [sum(chunks[:g]) for g in range(len(groups))]

    def chunk_bytes(g, c):
        two, one = groups[g]
        if c < len(two):
            ref = two[len(two) - 1 - c]
            return ref.shape[1] // 4 * ref.shape[2] * 2
        rest = sum(r.shape[1] * r.shape[2] * 2 for r in one[1:]) if c == chunks[g] - 1 else 0
        return one[0].shape[1] * one[0].shape[2] * 2 // q_parts[g] + rest

    def start_chunk(g, c, s, way):
        for r in pieces(g, c, shard(s - 1, way)):
            remote(r, r, zs.at[g, way, lax.rem(s, 4)], zr.at[first[g] + c, way, lax.rem(s, 4)],
                   {"sp": z_next if way == 0 else z_prev}).start()

    y_far = lax.rem(y + 2, 4)
    direct_from = n_right
    finals = (n_right + 1, n_right + 3, n_right + 3)

    def y_start(g, s, way, kind, q):
        up_way = kind == 0 or (kind == 2 and way == 0)
        k = kind // 2
        where = y_far if kind == 3 else (y_next if up_way else y_prev)
        for ref in groups[g][0]:
            r = part(ref, shard(s, way), q)
            if kind == 3:
                remote(r, r, yds.at[g], ydr.at[g], {"fs": where}).start()
            else:
                remote(r, r, ys.at[g, k, lax.rem(s, 4)], yr.at[g, k, s - 1],
                       {"fs": where}).start()

    def y_wait(sem, g, s, per_way):
        @pl.when(s <= n_left)
        def _():
            wait_bytes(sem, 2 * per_way * part_bytes[g])

        @pl.when(s > n_left)
        def _():
            wait_bytes(sem, per_way * part_bytes[g])

    def comm(g, s):
        for c in range(chunks[g]):
            for way in (0, 1):
                last = (n_right, n_left)[way]

                @pl.when((s >= 1) & (s <= last))
                def _():
                    wait_bytes(zr.at[first[g] + c, way, lax.rem(s, 4)], chunk_bytes(g, c))

                @pl.when(s < last)
                def _():
                    start_chunk(g, c, s + 1, way)

                if c == len(groups[g][0]) - 1:
                    @pl.when((s >= 1) & (s <= last))
                    def _():
                        y_start(g, s, way, 0, y)
                        y_start(g, s, way, 1, y)

                        @pl.when(s >= direct_from)
                        def _():
                            y_start(g, s, way, 3, y)

        @pl.when((s >= 3) & (s <= n_right + 2))
        def _():
            wait_bytes(zs.at[g, 0, lax.rem(s - 2, 4)], z_bytes[g])

            @pl.when(s - 2 <= n_left)
            def _():
                wait_bytes(zs.at[g, 1, lax.rem(s - 2, 4)], z_bytes[g])

    def share(g, s):
        lag = SHARE_LAGS[g]
        final = finals[g]

        @pl.when((s >= 1 + lag) & (s <= n_right + lag))
        def _():
            y_wait(yr.at[g, 0, s - lag - 1], g, s - lag, 2)
            y_wait(ys.at[g, 0, lax.rem(s - lag, 4)], g, s - lag, 2)

            @pl.when(s - lag < direct_from)
            def _():
                y_start(g, s - lag, 0, 2, y_prev)
                y_start(g, s - lag, 1, 2, y_next)

        @pl.when((s >= 2 + lag) & (s <= direct_from + lag))
        def _():
            wait_bytes(ys.at[g, 1, lax.rem(s - lag - 1, 4)], 2 * part_bytes[g])

        def complete(k, carry):
            @pl.when(k < direct_from)
            def _():
                wait_bytes(yr.at[g, 1, k - 1], 2 * part_bytes[g])

            @pl.when(k == direct_from)
            def _():
                wait_bytes(ydr.at[g], part_bytes[g])
                wait_bytes(yds.at[g], part_bytes[g])

            with jax.named_scope("mm"):
                multiply(g, k)
            return carry

        @pl.when((s >= 3 + lag) & (s <= final))
        def _():
            low, high = s - 2 - lag, jnp.where(s == final, n_right, s - 2 - lag)
            if g == 0:
                low = jnp.where(s == final, low + 1, low)
                high = jnp.where(s == final - 1, high + 1, high)
            lax.fori_loop(low, high + 1, complete, 0)

    def both(ref, j1, j2, axis):
        return jnp.concatenate([ref[j1], ref[j2]], axis=axis)

    def rows_at(k):
        j1 = jnp.where(k == n_right, z, shard(k, 0))
        j2 = shard(k, 1)
        return j1, j2, both(normed, j1, j2, 1)

    def multiply_early(k):
        j1, j2, rows = rows_at(k)
        acc_q[...] += jnp.dot(rows, both(aq, j1, j2, 0), preferred_element_type=F32)
        acc_s[:, :16] += lax.dot_general(
            rows, both(as_, j1, j2, 1), (((1,), (1,)), ((), ())), preferred_element_type=F32)

    def multiply(g, k):
        j1, j2, rows = rows_at(k)
        if g == 0:
            acc_a[...] += jnp.dot(rows, both(ap, j1, j2, 0), preferred_element_type=F32)
        elif g == 2:
            acc_g[...] += jnp.dot(rows[:t_rows], both(gp, j1, j2, 0), preferred_element_type=F32)
        else:
            w = jnp.concatenate([both(cp, j1, j2, 0), both(cq, j1, j2, 0)], axis=1)
            acc_c[...] += jnp.dot(rows, w, preferred_element_type=F32)

    edge_lanes = pl.ds(pl.multiple_of(tp * 256, 256), 256)

    def border():
        return remote(tok.at[pl.ds(t_rows - 32, 32), edge_lanes], tok_edge.at[:, edge_lanes],
                      hs.at[0], hr.at[0], {"sp": z_next})

    def border_share(i):
        ref = tok_edge.at[:, edge_lanes]
        return remote(ref, ref, hs.at[1], hr.at[1], {"tp": lax.rem(tp + i, 8)})

    def short_filter(source, lo, hi, kernel, target):
        weights = [kernel[k:k + 1, :].astype(F32) for k in range(4)]

        def strip(i, carry):
            block = source[pl.ds(pl.multiple_of(i * 64, 64), 72), lo:hi]
            total = weights[0] * pltpu.roll(block, 72 - 5, 0)[:64]
            for k in range(1, 4):
                total = total + weights[k] * pltpu.roll(block, 72 - 5 - k, 0)[:64]
            target[pl.ds(pl.multiple_of(i * 64, 64), 64), :] = (
                total * jax.nn.sigmoid(total)).astype(BF16)
            return carry

        lax.fori_loop(0, t_rows // 64, strip, 0)

    def extend(target, acc, lo, hi):
        target[0:8, :] = jnp.where(z > 0, acc[t_rows + 24:, lo:hi].astype(BF16).astype(F32), 0.0)
        target[8:, :] = acc[0:t_rows, lo:hi].astype(BF16).astype(F32)

    def finish_c():
        value = acc_c[:, :256].astype(BF16).astype(F32)
        sig = acc_c[:, 256:].astype(BF16).astype(F32)
        glu = (value * jax.nn.sigmoid(sig)).astype(BF16).astype(F32)
        ext31[0:32, :] = jnp.where(z > 0, glu[t_rows:], 0.0)
        ext31[32:, :] = glu[:t_rows]

    lane = lax.broadcasted_iota(jnp.int32, (1, 128), 1)

    def by_head(first, rows=slice(None)):
        c = cols_ref[rows, first:first + 4]
        return jnp.concatenate(
            [jnp.where(lane < 64, c[:, 2 * k:2 * k + 1], c[:, 2 * k + 1:2 * k + 2])
             for k in range(2)], axis=1)

    def local_rates():
        extend(extq, acc_q, 0, 256)
        short_filter(extq, 0, 128, f_wr, b_ref)
        short_filter(extq, 128, 256, f_rd, c_ref)
        head = lax.broadcasted_iota(jnp.int32, (8, t_rows), 0)
        place = lax.broadcasted_iota(jnp.int32, (8, t_rows), 1)
        bias8 = jnp.zeros((8, t_rows), F32)
        rate8 = jnp.zeros((8, t_rows), F32)
        for h in range(4):
            bias8 = jnp.where(head == h, bias[h], bias8)
            rate8 = jnp.where(head == h, rate[h], rate8)
        steps = acc_s[0:t_rows, :].astype(BF16).astype(F32).T[:8] + bias8
        steps = jnp.maximum(steps, 0.0) + jnp.log1p(jnp.exp(-jnp.abs(steps)))
        rows_ref[0:4, :] = shift[...]
        rows_ref[4:8, :] = jnp.zeros((4, t_rows), F32)
        total = rows_ref[0:8, :] - steps * jnp.exp(rate8)
        k = 1
        while k < t_rows:
            total = total + jnp.where(place >= k, pltpu.roll(total, k, 1), 0.0)
            k *= 2
        end = total[:, t_rows - 1:t_rows]
        rows_ref[0:8, :] = total
        rows_ref[8:16, :] = steps
        rows_ref[16:24, :] = steps * jnp.exp(end - total)
        rows_ref[24:32, :] = jnp.exp(total)
        rows_ref[32:, :] = jnp.zeros((96, t_rows), F32)
        cols_ref[...] = rows_ref[...].T
        spread = jnp.concatenate(
            [jnp.where(lane < 64, end[2 * k:2 * k + 1, :], end[2 * k + 1:2 * k + 2, :])
             for k in range(2)], axis=1)
        tbuf[z] = jnp.broadcast_to(spread, (8, 256))

    def local_state():
        extend(ext4, acc_a, 0, 256)
        short_filter(ext4, 0, 256, f_in, x_ref)
        scaled = (x_ref[...].astype(F32) * by_head(16)).astype(BF16)
        ebuf[z] = lax.dot_general(
            b_ref[...], scaled, (((0,), (0,)), ((), ())), preferred_element_type=F32
        ).astype(BF16)

    e_bytes = (2 * 32 * 256 + 4 * 8 * 256,) + (2 * 32 * 256,) * 3

    def state_start(c, s, way):
        j = shard(s - 1, way)
        where = {"sp": z_next if way == 0 else z_prev}
        for r in [ebuf.at[j, pl.ds(32 * c, 32)]] + [tbuf.at[j]] * (c == 0):
            remote(r, r, es.at[way, lax.rem(s, 2)], er.at[c, way, lax.rem(s, 4)], where).start()

    def state_ring(s):
        for c in range(4):
            for way in (0, 1):
                last = (n_right, n_left)[way]

                @pl.when(s <= last)
                def _():
                    wait_bytes(er.at[c, way, lax.rem(s, 4)], e_bytes[c])

                @pl.when(s < last)
                def _():
                    state_start(c, s + 1, way)

        for way in (0, 1):
            last = (n_right, n_left)[way]

            @pl.when(s <= last)
            def _():
                j = shard(s, way)
                total = tbuf[j][0:1]
                if way == 0:
                    @pl.when(z >= s)
                    def _():
                        e_right[...] += jnp.exp(run[0:1, :]) * ebuf[j].astype(F32)
                        run[...] += total
                else:
                    @pl.when(z + s >= n)
                    def _():
                        e_left[...] = e_left[...] * jnp.exp(total) + ebuf[j].astype(F32)
                wait_bytes(es.at[way, lax.rem(s, 2)], sum(e_bytes))

    def inside_strip(i):
        k = 128 * (i + 1)
        at = slice(128 * i, k)
        scores = lax.dot_general(
            c_ref[at, :], b_ref[0:k, :], (((1,), (1,)), ((), ())), preferred_element_type=F32)
        diag = (lax.broadcasted_iota(jnp.int32, (128, k), 0) + 128 * i
                >= lax.broadcasted_iota(jnp.int32, (128, k), 1))
        pieces = []
        for h in range(4):
            gap = cols_ref[at, h:h + 1] - rows_ref[h:h + 1, 0:k]
            decay = jnp.exp(jnp.where(diag, gap, -jnp.inf)) * rows_ref[8 + h:9 + h, 0:k]
            tile = slice(128 * (h // 2), 128 * (h // 2) + 128)
            pieces.append(jnp.dot((scores * decay).astype(BF16), x_ref[0:k, tile],
                                  preferred_element_type=F32))
        for k in range(2):
            gains = jnp.where(lane < 64, skip[2 * k], skip[2 * k + 1])
            lanes = slice(128 * k, 128 * k + 128)
            inside[at, lanes] = (jnp.where(lane < 64, pieces[2 * k], pieces[2 * k + 1])
                                 + gains * x_ref[at, lanes].astype(F32))

    def stat_copy(i):
        return remote(stat.at[tp], stat.at[tp], ss.at[0], sr.at[0], {"tp": lax.rem(tp + i, 8)})

    def long_filter(half):
        def strip(i, carry):
            block = ext31[pl.ds(pl.multiple_of(i * 64, 64), 96), :]
            total = jnp.zeros((8, 8, 256), F32)
            for r in range(8):
                moved = block if r == 0 else pltpu.roll(block, 96 - r, 0)
                for a in range(5):
                    k = 8 * a + r - 2
                    if 0 <= k < 31:
                        total = total + (tapsb[8 * k:8 * k + 8, :][None]
                                         * moved[8 * a:8 * a + 64].reshape(8, 8, 256))
            total = total.reshape(64, 256)
            at = pl.ds(pl.multiple_of(i * 64, 64), 64)
            filtered[at, :] = total
            sum1 = jnp.sum(total, axis=1, keepdims=True)
            sum2 = jnp.sum(total * total, axis=1, keepdims=True)
            sums_ref[at, :] = jnp.where(lane == 0, sum1, jnp.where(lane == 1, sum2, 0.0))
            return carry

        lax.fori_loop(half * (t_rows // 128), (half + 1) * (t_rows // 128), strip, 0)

    def send_sums():
        stat[tp] = sums_ref[...].T[0:8]
        for i in range(1, 8):
            stat_copy(i).start()

    def filter_act():
        with jax.named_scope("fact_wait"):
            wait_bytes(sr.at[0], 7 * 8 * t_rows * 4)
        sums = stat[0]
        for i in range(1, 8):
            sums = sums + stat[i]
        mean = sums[0:1] / CHANNELS
        var = sums[1:2] / CHANNELS - mean * mean
        rows_ref[32:33, :] = mean
        rows_ref[33:34, :] = lax.rsqrt(var + 1e-05)
        sums_ref[...] = rows_ref[...].T

        def strip(i, carry):
            at = pl.ds(pl.multiple_of(i * 64, 64), 64)
            f = (filtered[at, :] - sums_ref[at, 32:33]) * sums_ref[at, 33:34] * ch_gain[...]
            act[at, 256:512] = (f * jax.nn.sigmoid(f)).astype(BF16)
            return carry

        lax.fori_loop(0, t_rows // 64, strip, 0)
        wait_bytes(ss.at[0], 7 * 8 * t_rows * 4)

    own[0].wait()
    as_[z] = jnp.concatenate([ws_v[...].astype(F32), jnp.zeros((12, 128), F32)]).astype(BF16)
    for c in own[1:4]:
        c.wait()
    with jax.named_scope("entry"):
        pl.semaphore_wait(barrier, len(greet))
    for c in range(chunks[0]):
        start_chunk(0, c, 1, 0)
        start_chunk(0, c, 1, 1)
    for c in own[4:]:
        c.wait()

    border().start()

    def norm_rows(source, at, to):
        v = source[at, :].astype(F32)
        scale = lax.rsqrt(jnp.mean(v * v, axis=-1, keepdims=True) + 1e-06)
        v = (v * scale * gain[...]).astype(BF16)
        for j in range(n):
            normed[j, to, :] = v[:, j * 128:(j + 1) * 128]

    def norm_strip(i, carry):
        at = pl.ds(pl.multiple_of(i * 32, 32), 32)
        norm_rows(tok, at, at)
        return carry

    with jax.named_scope("norm"):
        lax.fori_loop(0, t_rows // 32, norm_strip, 0)
    e_right[...] = jnp.zeros_like(e_right)
    run[...] = jnp.zeros_like(run)
    e_left[...] = opening[...].reshape(256, 128).T
    for acc in (acc_a, acc_q, acc_s, acc_c, acc_g):
        acc[...] = jnp.zeros_like(acc)
    for k in range(taps.shape[0]):
        tapsb[8 * k:8 * k + 8, :] = jnp.broadcast_to(
            taps[k:k + 1, :].astype(F32), (8, 256))

    done = [f + o for f, o in zip(finals, OFFSETS)]
    state_at = done[0]
    long_at = done[1] + 1
    last_slot = max(max(done), state_at + n_right, state_at + 5, long_at + 2) + 1

    assert long_at + 1 < state_at + n_right and last_slot == state_at + n_right + 1

    def at_step(g, t):
        return t - OFFSETS[g] - (jnp.where(t > state_at, 0, 1) if g == 2 else 0)

    def slot(t, carry):
        @pl.when(t == state_at + n_right)
        def _():
            with jax.named_scope("fact"):
                filter_act()

        @pl.when((t > state_at) & (t <= state_at + n_right))
        def _():
            with jax.named_scope("ring"):
                state_ring(t - state_at)

        for g in range(3):
            s = at_step(g, t)
            low = 1 if g == 0 else 0

            @pl.when((s >= low) & (s <= n_right + 2))
            def _():
                with jax.named_scope("comm%d" % g):
                    comm(g, s)

        @pl.when(t == 1)
        def _():
            border().wait_recv()
            for i in range(1, 8):
                border_share(i).start()

        @pl.when(t == 3)
        def _():
            wait_bytes(hr.at[1], 7 * 32 * 256 * 2)
            norm_rows(tok_edge, pl.ds(0, 32), pl.ds(t_rows, 32))

        def early(k, carry):
            multiply_early(k)
            return carry

        @pl.when((t >= 3) & (t <= n_right))
        def _():
            with jax.named_scope("mmq"):
                lax.fori_loop(jnp.where(t == 3, 1, t), t + 1, early, 0)

        @pl.when(t == n_right + 1)
        def _():
            with jax.named_scope("rates"):
                local_rates()

        for i in range(4):
            @pl.when(t == state_at + 1 + i)
            def _():
                with jax.named_scope("inside"):
                    inside_strip(i)

        for i in range(2):
            @pl.when(t == long_at + i)
            def _():
                with jax.named_scope("longf"):
                    long_filter(i)
                    if i == 1:
                        send_sums()

        for g in range(3):
            s = at_step(g, t)

            @pl.when((s >= 2) & (s <= finals[g]))
            def _():
                with jax.named_scope("share%d" % g):
                    share(g, s)

        @pl.when(t == state_at)
        def _():
            with jax.named_scope("lstate"):
                local_state()
            for c in range(4):
                for way in (0, 1):
                    state_start(c, 1, way)
            with jax.named_scope("extra"):
                comm(2, state_at - OFFSETS[2])
                share(2, state_at - OFFSETS[2])

        @pl.when(t == done[1])
        def _():
            with jax.named_scope("fin_c"):
                finish_c()
        return carry

    lax.fori_loop(1, last_slot, slot, 0)
    border().wait_send()
    wait_bytes(hs.at[1], 7 * 32 * 256 * 2)

    entering = (e_left[...] * jnp.exp(run[0:1, :]) + e_right[...]).astype(BF16)
    for i in range(4):
        at = slice(128 * i, 128 * i + 128)
        carried = jnp.dot(c_ref[at, :], entering, preferred_element_type=F32)
        v = inside[at, :] + by_head(24, at) * carried
        g = acc_g[at, :].astype(BF16).astype(F32)
        v = v * (g * jax.nn.sigmoid(g))
        v = v * lax.rsqrt(jnp.mean(v * v, axis=-1, keepdims=True) + 1e-06)
        act[at, 0:256] = (v * out_gain[...]).astype(BF16)

    blocks = CHANNELS // 256

    def rows_of(xx, cc):
        return pl.ds(pl.multiple_of((2 * xx + cc) * 64, 64), 64)

    def at_x(k):
        return {"tp": 2 * lax.rem(x + k, 4) + core}

    def pair_copy(b):
        return remote(d2d_src.at[b], d2d_dst.at[b], os_.at[0], or_.at[0, b],
                      {"tp": 2 * x + 1 - core})

    def far_copy(b):
        return remote(far_src.at[b], far_dst.at[b], os_.at[1], or_.at[1, b],
                      at_x(1 + 2 * lax.rem(b, 2)))

    def relay_copy(b):
        return remote(rn_src.at[b], rn_dst.at[b], os_.at[2], or_.at[2, b],
                      at_x(1 + 2 * lax.rem(b, 2)))

    def direct_copy(b):
        return remote(dn_src.at[b], dn_dst.at[b], os_.at[3], or_.at[3, b],
                      at_x(3 + 2 * lax.rem(b, 2)))

    def stage_multiply(b):
        w = jnp.concatenate(
            [both(up, 2 * b, 2 * b + 1, 1), both(uq, 2 * b, 2 * b + 1, 1)], axis=0)
        pbuf[b] = jnp.dot(act[...], w, preferred_element_type=F32)
        for xx in range(4):
            d2d_src[b, xx] = pbuf[b, rows_of(xx, 1 - core), :].astype(BF16)
        pair_copy(b).start()

    def stage_pair(b):
        pair_copy(b).wait_recv()
        for xx in range(4):
            at = rows_of(xx, core)
            pbuf[b, at, :] = pbuf[b, at, :] + d2d_dst[b, xx].astype(F32)
        far_src[b] = pbuf[b, rows_of(lax.rem(x + 2, 4), core), :].astype(BF16)
        far_copy(b).start()

    def stage_direct(b):
        dn_src[b] = pbuf[b, rows_of(lax.rem(x + 3 + 2 * lax.rem(b, 2), 4), core), :].astype(BF16)
        direct_copy(b).start()

    def stage_relay(b):
        far_copy(b).wait_recv()
        mine = pbuf[b, rows_of(lax.rem(x + 1 + 2 * lax.rem(b, 2), 4), core), :]
        rn_src[b] = (mine + far_dst[b].astype(F32)).astype(BF16)
        relay_copy(b).start()

    def stage_out(b):
        relay_copy(b).wait_recv()
        direct_copy(b).wait_recv()
        total = (pbuf[b, rows_of(x, core), :] + rn_dst[b].astype(F32)) + dn_dst[b].astype(F32)
        out[0, :, pl.ds(pl.multiple_of(b * 256, 256), 256)] = total.astype(BF16)

    def out_slot(i, carry):
        @pl.when(i < blocks)
        def _():
            with jax.named_scope("o_mm"):
                stage_multiply(i)

        for lag, stage in ((3, stage_pair), (9, stage_direct), (10, stage_relay), (18, stage_out)):
            @pl.when((i >= lag) & (i < blocks + lag))
            def _():
                with jax.named_scope("o_st%d" % lag):
                    stage(i - lag)
        return carry

    lax.fori_loop(0, blocks + 18, out_slot, 0)
    with jax.named_scope("o_end"):
        for k, r in enumerate((d2d_src, far_src, rn_src, dn_src)):
            pltpu.make_async_copy(r, r, os_.at[k]).wait()


def per_device(
    tokens, input_gain, weight_gate, weight_input, weight_write, weight_read, weight_step,
    weight_value, weight_sigmoid, filter_input, filter_write, filter_read, step_bias, rate_log,
    skip_gain, output_gain, opening_state, decay_shift, depth_filter, channel_gain,
    unproject_state, unproject_filter,
):
    n = lax.axis_size("sp")
    t = tokens.shape[1]
    hb = pl.BlockSpec(memory_space=pl.ANY)
    dma = pltpu.SemaphoreType.DMA
    steps = n // 2
    v = pltpu.VMEM
    return pl.pallas_call(
        partial(mixer_kernel, n),
        out_shape=jax.ShapeDtypeStruct((1, t // 8, CHANNELS), BF16),
        in_specs=[hb] * 22,
        out_specs=pl.BlockSpec(memory_space=pltpu.VMEM),
        scratch_shapes=[
            v((t, 2048), BF16), v((1, 2048), F32), v((4, 128), BF16),
            v((4, 256), BF16), v((4, 128), BF16), v((4, 128), BF16),
            *[pltpu.SMEM((4,), F32)] * 3,
            v((1, 256), F32), v((4, 64, 128), F32), v((4, t), F32), v((31, 256), BF16),
            v((1, 256), F32),
            v((n, t + 32, 128), BF16),
            v((n, 128, 256), BF16), v((n, 128, 256), BF16), v((n, 16, 128), BF16),
            v((n, 128, 384), BF16), v((n, 128, 128), BF16), v((n, 448, 128), BF16), v((n, 64, 128), BF16),
            v((n, 128, 256), BF16),
            v((t + 32, 256), F32), v((t + 32, 256), F32), v((t + 32, 128), F32), v((t + 32, 512), F32),
            v((t, 256), F32),
            v((384, 128), F32), v((31 * 8, 256), F32),
            v((32, 2048), BF16),
            v((8 + t, 256), F32), v((8 + t, 256), F32), v((32 + t, 256), F32),
            v((t, 256), BF16), v((t, 128), BF16), v((t, 128), BF16),
            v((128, t), F32), v((t, 128), F32), v((t, 256), F32), v((t, 256), F32),
            v((t, 128), F32),
            v((8, 8, t), F32), v((n, 128, 256), BF16), v((n, 8, 256), F32),
            v((128, 256), F32), v((128, 256), F32), v((8, 256), F32), v((t, 512), BF16),
            v((8, t, 256), F32), v((8, 4, 64, 256), BF16), v((8, 4, 64, 256), BF16),
            *[v((8, 64, 256), BF16)] * 6,
            dma((24,)), dma((3, 2, 4)), dma((11, 2, 4)),
            dma((3, 2, 4)), dma((3, 2, steps)), dma((3,)), dma((3,)),
            dma((2, 2)), dma((4, 2, 4)), dma((2,)), dma((2,)),
            dma((1,)), dma((1,)), dma((4,)), dma((4, 8)),
        ],
        compiler_params=pltpu.CompilerParams(
            collective_id=0, has_side_effects=True, vmem_limit_bytes=62 * 1024 * 1024),
        name="mixer",
    )(
        tokens, input_gain.reshape(1, -1), weight_input, weight_write, weight_step.T, weight_gate,
        weight_read, weight_value, weight_sigmoid, unproject_state, unproject_filter,
        filter_input, filter_write, filter_read, step_bias, rate_log, skip_gain,
        output_gain.reshape(1, -1), opening_state, decay_shift, depth_filter,
        channel_gain.reshape(1, -1),
    )


def solution(mesh):
    in_specs = (
        P("fs", "sp", None),
        P(),
        P("sp", "tp"),
        P("sp", "tp"),
        P("sp", "tp"),
        P("sp", "tp"),
        P("sp", "tp"),
        P("sp", "tp"),
        P("sp", "tp"),
        P(None, "tp"),
        P(None, "tp"),
        P(None, "tp"),
        P("tp"),
        P("tp"),
        P("tp"),
        P("tp"),
        P("fs", "tp", None, None),
        P("fs", "tp", "sp"),
        P(None, "tp"),
        P("tp"),
        P("tp", "sp"),
        P("tp", "sp"),
    )
    out_specs = P("fs", ("sp", "tp"), None)
    return jax.shard_map(
        per_device, mesh=mesh, in_specs=in_specs, out_specs=out_specs, check_vma=False
    )
```
